32 devices in a mesh: grp: 2 (over y), ra: 4 (over z), cb: 4 (over x, core).
Axes of the slice: x: 2, y: 2, z: 4, core: 2. Of those that a mesh axis runs over, the one named last changes fastest.
Arguments:
- tokens: bfloat16 [1024, 4096], P('grp', 'ra'), parts along dimension 0, may hold values from -14 to 14
- pre_gain: bfloat16 [2, 4096], P(None, 'ra'), may hold values from 0.099609375 to 1.8984375
- post_gain: bfloat16 [2, 4096], P(None, 'ra'), may hold values from 0.099609375 to 1.8984375
- gate_weight: bfloat16 [2, 4096, 11008], P(None, 'ra', 'cb'), may hold values from -0.09375 to 0.09375
- up_weight: bfloat16 [2, 4096, 11008], P(None, 'ra', 'cb'), may hold values from -0.09375 to 0.09375
- gate_taps: bfloat16 [2, 3, 11008], P(None, None, 'cb'), may hold values from -3 to 3
- up_taps: bfloat16 [2, 3, 11008], P(None, None, 'cb'), may hold values from -3 to 3
- gate_bias: bfloat16 [2, 11008], P(None, 'cb'), may hold values from -3 to 3
- up_bias: bfloat16 [2, 11008], P(None, 'cb'), may hold values from -3 to 3
- down_weight: bfloat16 [2, 11008, 4096], P(None, 'cb', 'ra'), may hold values from -0.07624929 to 0.07624929
Outputs:
- layer_out: bfloat16 [1024, 4096], P('grp', 'ra'), parts along dimension 0
The draws below stay inside these ranges and needn't reach their ends.
There are 2 independent parts, one for each index of `grp`. The reference program is written for one: setup_inputs(seed, part) draws one part's arguments, and reference() takes and returns one part's arrays. A program takes and returns all parts, laid end to end along the dimension named above; an argument that names none is the same for every part. Nothing has to cross between parts.
All inputs are finite; a program needn't handle non-finite values.
Results may differ from the reference program's by a relative error of at most 0.024.
Values may be sent and summed in bfloat16 or wider, within the bound.
A program may use at most 128 MiB of HBM per device.

```python
import jax
import jax.numpy as jnp
from jax import lax

D = 4096
FF = 11008
TAPS = 3
LAYERS = 2
SEQS = 2
TOKENS = 512
HID_BLOCK = 2752
N_CB = 4


def draw_tokens(key, part):
    key_rows, key_cols, key_vals = jax.random.split(jax.random.fold_in(key, 11), 3)
    position = jnp.arange(D, dtype=jnp.float32)[None, :] / D
    row_log = jax.random.uniform(key_rows, (TOKENS, 1), jnp.float32, -0.5, 0.5) * jnp.log(10.0)
    col_log = (0.5 * position + 0.5 * jax.random.uniform(key_cols, (1, D), jnp.float32) - 0.5) * jnp.log(10.0)
    entries = jnp.clip(jax.random.normal(key_vals, (TOKENS, D), jnp.float32), -4.0, 4.0)
    return (entries * jnp.exp(row_log) * jnp.exp(col_log) / 3.0).astype(jnp.bfloat16)


def draw_down_weight(key, part):
    key_cols, key_vals = jax.random.split(jax.random.fold_in(key, 23), 2)
    position = jnp.arange(D, dtype=jnp.float32)[None, None, :] / D
    spread = jax.random.uniform(key_cols, (LAYERS, 1, D), jnp.float32)
    col_log = (0.5 * position + 0.5 * spread - 0.5) * jnp.log(10.0)
    entries = jnp.clip(jax.random.normal(key_vals, (LAYERS, FF, D), jnp.float32), -2.5, 2.5)
    return (entries * jnp.exp(col_log) / jnp.sqrt(jnp.float32(FF))).astype(jnp.bfloat16)


def level_of(rng, extent, cuts, least, top_value):
    level, own = 1.0, jax.random.fold_in(rng, 6)
    for axis_at, parts in cuts:
        steps = jnp.exp(jax.random.uniform(jax.random.fold_in(own, axis_at), (parts,), jnp.float32, least / len(cuts), top_value / len(cuts)))
        level = level * jnp.repeat(steps, extent[axis_at] // parts).reshape([-1 if axis == axis_at else 1 for axis in range(len(extent))])
    return level


def bell_draw(stream_key, extent, scale, bound, shards=(), kind=jnp.bfloat16):
    values = jax.random.normal(stream_key, extent, jnp.float32) * scale
    if len(shards) > 0:
        values = level_of(stream_key, extent, shards, -0.22, 0.18) * values
    return jnp.clip(values, min=-bound, max=bound).astype(kind)


def setup_inputs(seed: int = 0, part: int = 0) -> dict:
    key_of = jax.random.split(jax.random.key(seed), 11)
    part_splits = jax.random.split(jax.random.fold_in(key_of[10], part), 11)
    tokens = draw_tokens(jax.random.fold_in(jax.random.fold_in(key_of[10], part), 71), part)
    pre_gain = jnp.clip(1.0 + 0.18 * jax.random.normal(key_of[1], (LAYERS, D), jnp.float32), 0.099609375, 1.8984375).astype(jnp.bfloat16)
    post_gain = jnp.clip(1.0 + 0.18 * jax.random.normal(key_of[2], (LAYERS, D), jnp.float32), 0.099609375, 1.8984375).astype(jnp.bfloat16)
    gate_weight = bell_draw(key_of[3], (LAYERS, D, FF), D ** -0.5, 0.09375, ((1, 4), (2, 4)))
    up_weight = bell_draw(key_of[4], (LAYERS, D, FF), D ** -0.5, 0.09375, ((1, 4), (2, 4)))
    gate_taps = bell_draw(key_of[5], (LAYERS, TAPS, FF), 0.577, 3.0, ((2, 4),))
    up_taps = bell_draw(key_of[6], (LAYERS, TAPS, FF), 0.577, 3.0, ((2, 4),))
    gate_bias = bell_draw(key_of[7], (LAYERS, FF), 0.5, 3.0, ((1, 4),))
    up_bias = bell_draw(key_of[8], (LAYERS, FF), 0.5, 3.0, ((1, 4),))
    down_weight = draw_down_weight(jax.random.fold_in(key_of[10], 71), part)
    return dict(tokens=tokens, pre_gain=pre_gain, post_gain=post_gain, gate_weight=gate_weight, up_weight=up_weight, gate_taps=gate_taps, up_taps=up_taps, gate_bias=gate_bias, up_bias=up_bias, down_weight=down_weight)


epsilon = 1e-06
residual_scale = 0.5

def shift_rows(values, delay_by, sequences):
    total_rows, columns = values.shape
    per_sequence = total_rows // sequences
    grouped = values.reshape(sequences, per_sequence, columns)
    moved = jnp.pad(grouped, ((0, 0), (delay_by, 0), (0, 0)))[:, :per_sequence]
    return moved.reshape(total_rows, columns)

def causal_conv(values, tap_weights, sequences):
    tap_count = tap_weights.shape[0]
    result = tap_weights[tap_count - 1] * values
    for offset in range(1, tap_count):
        result = result + tap_weights[tap_count - 1 - offset] * shift_rows(values, offset, sequences)
    return result

def reference(tokens, pre_gain, post_gain, gate_weight, up_weight, gate_taps, up_taps, gate_bias, up_bias, down_weight):
    state = tokens
    for which_layer in range(LAYERS):
        widened = state.astype(jnp.float32)
        pre_scale = lax.rsqrt(lax.optimization_barrier(jnp.sum(widened * widened, axis=1, keepdims=True)) / D + epsilon)
        normed = (widened * pre_gain[which_layer].astype(jnp.float32)).astype(jnp.bfloat16)
        gate_lin = jnp.dot(normed, gate_weight[which_layer], preferred_element_type=jnp.float32) * pre_scale
        up_lin = jnp.dot(normed, up_weight[which_layer], preferred_element_type=jnp.float32) * pre_scale
        gate_conv = causal_conv(gate_lin, gate_taps[which_layer].astype(jnp.float32), SEQS) + gate_bias[which_layer].astype(jnp.float32)
        up_conv = causal_conv(up_lin, up_taps[which_layer].astype(jnp.float32), SEQS) + up_bias[which_layer].astype(jnp.float32)
        hidden = (jax.nn.gelu(gate_conv, approximate=True) * up_conv).astype(jnp.bfloat16)
        blocks = hidden.reshape(TOKENS, N_CB, HID_BLOCK).astype(jnp.float32)
        weights = down_weight[which_layer].reshape(N_CB, HID_BLOCK, D).astype(jnp.float32)
        partials = jnp.einsum('tkf,kfd->ktd', blocks, weights).astype(jnp.bfloat16)
        branch = lax.optimization_barrier(jnp.sum(partials.astype(jnp.float32), axis=0))
        post_scale = lax.rsqrt(lax.optimization_barrier(jnp.sum(branch * branch, axis=1, keepdims=True)) / D + epsilon)
        state = (residual_scale * widened + branch * post_scale * post_gain[which_layer].astype(jnp.float32)).astype(jnp.bfloat16)
    return state
```

```python
import functools

import jax
import jax.numpy as jnp
from jax import lax
from jax.experimental import pallas as pl
from jax.experimental.pallas import tpu as pltpu
from jax.sharding import PartitionSpec as P

LEN = 256
LANES = 128
BLOCK = 128
HALO = 8
SKEW = 3

epsilon = 1e-06
residual_scale = 0.5
MESH = pl.DeviceIdType.MESH


class Plan:
    def __init__(self, layers, n, nx, tokens, dl, fl):
        self.layers, self.n, self.nx = layers, n, nx
        self.tokens, self.dl, self.fl = tokens, dl, fl
        self.nfull = fl // LANES
        self.nch = -(-fl // LANES)
        self.tail = fl - self.nfull * LANES
        self.blocks = tokens // BLOCK
        self.per_seq = LEN // BLOCK
        self.span = -(-self.nch // 2)
        self.half = BLOCK // 2
        self.stages = layers * self.blocks
        self.turn = (n - 1) * SKEW
        self.done = 2 * self.turn
        self.pair_at = self.done + 1
        self.x_at = self.pair_at + 3
        self.norm_at = self.x_at + 2
        self.next_at = self.norm_at + 1
        self.period = max(
            self.blocks * self.span,
            self.span + self.next_at + 1,
            (self.blocks - 1) * self.span + self.turn + 2,
        )
        self.steps = (layers - 1) * self.period + self.blocks * self.span + self.next_at + 1


def body_kernel(
    plan,
    state_hbm, pre_ref, post_ref, coef_ref, wg_hbm, wu_hbm, wd_hbm,
    out_ref,
    w, wd, part, hid, halo, acc, states, normed, scale, branch, pair_out, pair_in, xbuf, pre_sq, post_sq,
    ssem, wsem, wtail, wdsem, part_send, part_recv, hid_send, hid_recv,
    pre_send, pre_recv, post_send, post_recv, x_send, x_recv, pair_send, pair_recv,
    back_send, back_recv,
):
    z = lax.axis_index("ra")
    k = lax.axis_index("cb")
    core, xi = k % 2, k // 2
    peer = k + 1 - 2 * core
    n, nx, layers, dl, fl = plan.n, plan.nx, plan.layers, plan.dl, plan.fl
    nch, nfull, tail, blocks, span, half = (
        plan.nch, plan.nfull, plan.tail, plan.blocks, plan.span, plan.half)
    width = dl * n
    f32 = jnp.float32

    def w_copies(layer, c):
        cols = pl.ds(pl.multiple_of(c * LANES, LANES), LANES)
        return (
            pltpu.make_async_copy(
                wg_hbm.at[layer, cols], w.at[c, pl.ds(0, LANES)], wsem.at[0, c]),
            pltpu.make_async_copy(
                wu_hbm.at[layer, cols], w.at[c, pl.ds(LANES, LANES)], wsem.at[1, c]),
        )

    def tail_copies(layer):
        cols = pl.ds(nfull * LANES, tail)
        return (
            pltpu.make_async_copy(
                wg_hbm.at[layer, cols], w.at[nfull, pl.ds(0, tail)], wtail.at[0]),
            pltpu.make_async_copy(
                wu_hbm.at[layer, cols], w.at[nfull, pl.ds(LANES, tail)], wtail.at[1]),
        )

    def w_do(layer, c, act):
        @pl.when(c < nfull)
        def _():
            for copy in w_copies(layer, c):
                act(copy)

        if tail:
            @pl.when(c == nfull)
            def _():
                for copy in tail_copies(layer):
                    act(copy)

    def start(copy):
        copy.start()

    def wait(copy):
        copy.wait()

    def wd_copy(layer):
        return pltpu.make_async_copy(
            wd_hbm.at[layer], wd.at[layer, pl.ds(0, fl)], wdsem.at[layer])

    def block_rows(b):
        return pl.ds(pl.multiple_of(b * BLOCK, BLOCK), BLOCK)

    def half_rows(b, which):
        return pl.ds(pl.multiple_of(b * BLOCK + which * half, half), half)

    def state_copy(b):
        return pltpu.make_async_copy(
            state_hbm.at[block_rows(b)], states.at[0, block_rows(b)], ssem.at[b])

    barrier = pltpu.get_barrier_semaphore()

    @pl.loop(1, n)
    def _(o):
        pl.semaphore_signal(
            barrier, inc=1, device_id={"ra": (z + o) % n}, device_id_type=MESH)

    pl.semaphore_signal(barrier, inc=1, device_id={"cb": peer}, device_id_type=MESH)
    for o in range(1, nx):
        pl.semaphore_signal(
            barrier, inc=1, device_id={"cb": (xi + o) % nx * 2 + core}, device_id_type=MESH)

    for b in range(blocks):
        state_copy(b).start()

    @pl.loop(0, nch)
    def _(c):
        w_do(0, c, start)

    for layer in range(layers):
        wd_copy(layer).start()

    def eye(rows):
        shape = (rows, LANES)
        return lax.broadcasted_iota(jnp.int32, shape, 0) == lax.broadcasted_iota(
            jnp.int32, shape, 1)

    def to_row(column):
        return jnp.sum(jnp.where(eye(column.shape[0]), column, 0.0), axis=0, keepdims=True)

    def to_column(row, rows):
        return jnp.sum(jnp.where(eye(rows), row, 0.0), axis=1, keepdims=True)

    def sq_copy(buf, send, recv, t, o, slot):
        return pltpu.make_async_remote_copy(
            src_ref=buf.at[t, slot], dst_ref=buf.at[t, slot],
            send_sem=send.at[t, o], recv_sem=recv.at[t, slot],
            device_id={"ra": (z + o) % n}, device_id_type=MESH)

    def sq_start(buf, send, recv, t):
        @pl.loop(1, n)
        def _(o):
            sq_copy(buf, send, recv, t, o, z).start()

    def sq_wait(buf, send, recv, t):
        @pl.loop(1, n)
        def _(o):
            sq_copy(buf, send, recv, t, o, (z + o) % n).wait_recv()

    def scale_of(buf, t, rows):
        total = buf[t, 0, 0:1, :]
        for slot in range(1, n):
            total = total + buf[t, slot, 0:1, :]
        return to_column(lax.rsqrt(total / width + epsilon), rows)

    def norm(layer, b):
        t = layer * blocks + b
        wide = states[layer, block_rows(b), :].astype(f32)
        normed[block_rows(b), :] = (wide * pre_ref[pl.ds(layer, 1), :]).astype(normed.dtype)
        row = to_row(jnp.sum(wide * wide, axis=1, keepdims=True))
        pre_sq[t, z] = jnp.broadcast_to(row, pre_sq.shape[2:])

    if tail:
        for lo in (0, LANES):
            w[nfull, lo + tail : lo + LANES, :] = jnp.zeros((LANES - tail, dl), w.dtype)
        for layer in range(layers):
            wd[layer, fl:, :] = jnp.zeros((nch * LANES - fl, dl), wd.dtype)

    state_copy(0).wait()
    norm(0, 0)
    pl.semaphore_wait(barrier, n - 1 + nx)
    sq_start(pre_sq, pre_send, pre_recv, 0)

    def place(d):
        if d == 0:
            return n - 1 - z, z - 1, z + 1
        return z, z + 1, z - 1

    def part_copy(d, t, j, target):
        return pltpu.make_async_remote_copy(
            src_ref=part.at[d, t, j], dst_ref=part.at[d, t, j],
            send_sem=part_send.at[d, t, j], recv_sem=part_recv.at[d, t, j],
            device_id={"ra": target}, device_id_type=MESH)

    def hid_copy(d, t, j, target):
        return pltpu.make_async_remote_copy(
            src_ref=hid.at[d, t, j], dst_ref=hid.at[d, t, j],
            send_sem=hid_send.at[d, t, j], recv_sem=hid_recv.at[d, t, j],
            device_id={"ra": target}, device_id_type=MESH)

    def decode(g):
        live = g >= 0
        g = jnp.maximum(g, 0)
        layer = g // plan.period
        rest = g - layer * plan.period
        b = rest // span
        j = rest - b * span
        return live & (layer < layers) & (b < blocks), layer, b, j

    def chunk_of(d, b, j):
        return 2 * j + (d + b // plan.per_seq) % 2

    def conv(values, before, taps, bias):
        rows = lax.broadcasted_iota(jnp.int32, before.shape, 0)
        count = len(taps)
        result = taps[count - 1] * values
        for offset in range(1, count):
            moved = pltpu.roll(values, offset, 0)
            head = jnp.where(rows < offset, pltpu.roll(before, offset, 0), moved[:HALO])
            moved = jnp.concatenate([head, moved[HALO:]], axis=0)
            result = result + taps[count - 1 - offset] * moved
        return result + bias

    def add_down(d, layer, b, j, c):
        wrows = pl.ds(pl.multiple_of(c * LANES, LANES), LANES)
        acc[block_rows(b), :] += jnp.dot(
            hid[d, layer * blocks + b, j], wd[layer, wrows, :], preferred_element_type=f32)

    def pair_copy(t):
        return pltpu.make_async_remote_copy(
            src_ref=pair_out, dst_ref=pair_in.at[t],
            send_sem=pair_send.at[t], recv_sem=pair_recv.at[t],
            device_id={"cb": peer}, device_id_type=MESH)

    def x_copy(t, o, slot):
        return pltpu.make_async_remote_copy(
            src_ref=xbuf.at[t, slot], dst_ref=xbuf.at[t, slot],
            send_sem=x_send.at[t, o], recv_sem=x_recv.at[t, slot],
            device_id={"cb": (xi + o) % nx * 2 + core}, device_id_type=MESH)

    def back_copy(layer, b, which):
        rows = half_rows(b, which)
        t = layer * blocks + b
        return pltpu.make_async_remote_copy(
            src_ref=states.at[layer + 1, rows], dst_ref=states.at[layer + 1, rows],
            send_sem=back_send.at[t], recv_sem=back_recv.at[t],
            device_id={"cb": peer}, device_id_type=MESH)

    @pl.loop(0, plan.steps)
    def _(s):
        @pl.when((s >= 1) & (s < blocks))
        def _():
            state_copy(s).wait()
            norm(0, s)
            sq_start(pre_sq, pre_send, pre_recv, s)

        live, layer, b, j = decode(s - plan.turn)

        @pl.when(live & (j == 0))
        def _():
            t = layer * blocks + b

            @pl.when(b == 0)
            def _():
                wd_copy(layer).wait()

            sq_wait(pre_sq, pre_send, pre_recv, t)
            scale[block_rows(b), :] = scale_of(pre_sq, t, BLOCK)
            acc[block_rows(b), :] = jnp.zeros((BLOCK, dl), f32)

        for d in range(2):
            p, nxt, prv = place(d)
            live, layer, b, j = decode(s - p * SKEW)
            c = chunk_of(d, b, j)
            t = layer * blocks + b

            @pl.when(live & (c < nch))
            def _():
                @pl.when(b == 0)
                def _():
                    w_do(layer, c, wait)

                own = lax.dot_general(
                    normed[block_rows(b), :], w[c], (((1,), (1,)), ((), ())),
                    preferred_element_type=f32)

                @pl.when(p == 0)
                def _():
                    part[d, t, j, 0] = own[:, :LANES].astype(part.dtype)
                    part[d, t, j, 1] = own[:, LANES:].astype(part.dtype)
                    part_copy(d, t, j, nxt).start()

                @pl.when((p > 0) & (p < n - 1))
                def _():
                    part_copy(d, t, j, nxt).wait_recv()
                    for i in range(2):
                        mine = own[:, i * LANES : (i + 1) * LANES]
                        part[d, t, j, i] = (part[d, t, j, i].astype(f32) + mine).astype(part.dtype)
                    part_copy(d, t, j, nxt).start()

                @pl.when(p == n - 1)
                def _():
                    part_copy(d, t, j, prv).wait_recv()
                    coef = coef_ref[layer, :, pl.ds(pl.multiple_of(c * LANES, LANES), LANES)]
                    m = coef.shape[0] // 2
                    row = [coef[i : i + 1, :] for i in range(2 * m)]
                    first = b % plan.per_seq == 0
                    sides = []
                    for i in range(2):
                        mine = own[:, i * LANES : (i + 1) * LANES]
                        total = (part[d, t, j, i].astype(f32) + mine) * scale[block_rows(b), :]
                        before = jnp.where(first, 0.0, halo[d, j, i])
                        halo[d, j, i] = total[BLOCK - HALO :, :]
                        sides.append(
                            conv(total, before, row[i * m : i * m + m - 1], row[i * m + m - 1]))
                    gate, up = sides
                    hid[d, t, j] = (jax.nn.gelu(gate, approximate=True) * up).astype(hid.dtype)
                    hid_copy(d, t, j, prv).start()
                    add_down(d, layer, b, j, c)

                @pl.when((b == blocks - 1) & (layer + 1 < layers))
                def _():
                    w_do(layer + 1, c, start)

        for d in range(2):
            p, nxt, prv = place(d)
            live, layer, b, j = decode(s - (plan.done - p * SKEW))
            c = chunk_of(d, b, j)
            t = layer * blocks + b

            @pl.when(live & (p < n - 1) & (c < nch))
            def _():
                hid_copy(d, t, j, nxt).wait_recv()

                @pl.when(p > 0)
                def _():
                    hid_copy(d, t, j, prv).start()

                add_down(d, layer, b, j, c)

        live, layer, b, j = decode(s - plan.done)

        @pl.when(live & (j == span - 1))
        def _():
            t = layer * blocks + b
            pair_out[...] = acc[half_rows(b, 1 - core), :].astype(pair_out.dtype)
            pair_copy(t).start()

        live, layer, b, j = decode(s - plan.pair_at)

        @pl.when(live & (j == span - 1))
        def _():
            t = layer * blocks + b
            pair_copy(t).wait()
            xbuf[t, xi] = (
                acc[half_rows(b, core), :] + pair_in[t].astype(f32)).astype(xbuf.dtype)
            for o in range(1, nx):
                x_copy(t, o, xi).start()

        live, layer, b, j = decode(s - plan.x_at)

        @pl.when(live & (j == span - 1))
        def _():
            t = layer * blocks + b
            for o in range(1, nx):
                x_copy(t, o, (xi + o) % nx).wait_recv()
            total = xbuf[t, 0].astype(f32)
            for i in range(1, nx):
                total = total + xbuf[t, i].astype(f32)
            branch[...] = total
            row = to_row(jnp.sum(total * total, axis=1, keepdims=True))
            post_sq[t, z] = jnp.broadcast_to(row, post_sq.shape[2:])
            sq_start(post_sq, post_send, post_recv, t)

        live, layer, b, j = decode(s - plan.norm_at)

        @pl.when(live & (j == span - 1))
        def _():
            t = layer * blocks + b
            sq_wait(post_sq, post_send, post_recv, t)
            rows = half_rows(b, core)
            states[layer + 1, rows, :] = (
                residual_scale * states[layer, rows, :].astype(f32)
                + branch[...] * scale_of(post_sq, t, half) * post_ref[pl.ds(layer, 1), :]
            ).astype(states.dtype)
            back_copy(layer, b, core).start()

        live, layer, b, j = decode(s - plan.next_at)

        @pl.when(live & (j == span - 1))
        def _():
            t = layer * blocks + b
            back_copy(layer, b, 1 - core).wait_recv()

            @pl.when(layer + 1 < layers)
            def _():
                norm(layer + 1, b)
                sq_start(pre_sq, pre_send, pre_recv, t + blocks)

            @pl.when(layer + 1 == layers)
            def _():
                out_ref[block_rows(b), :] = states[layers, block_rows(b), :]

    @pl.loop(0, plan.stages)
    def _(t):
        layer = t // blocks
        back_copy(layer, t - layer * blocks, core).wait_send()
        for o in range(1, nx):
            x_copy(t, o, xi).wait_send()

        @pl.loop(1, n)
        def _(o):
            sq_copy(pre_sq, pre_send, pre_recv, t, o, z).wait_send()
            sq_copy(post_sq, post_send, post_recv, t, o, z).wait_send()

        for d in range(2):
            p, nxt, prv = place(d)

            @pl.loop(0, span)
            def _(j):
                b = t - layer * blocks

                @pl.when(chunk_of(d, b, j) < nch)
                def _():
                    @pl.when(p < n - 1)
                    def _():
                        part_copy(d, t, j, nxt).wait_send()

                    @pl.when(p > 0)
                    def _():
                        hid_copy(d, t, j, prv).wait_send()


def run(plan, state, pre, post, coef, gate_weight, up_weight, down_weight):
    vmem = pl.BlockSpec(memory_space=pltpu.VMEM)
    hbm = pl.BlockSpec(memory_space=pl.ANY)
    dma = pltpu.SemaphoreType.DMA
    bf16, f32 = jnp.bfloat16, jnp.float32
    n, nx, dl, nch, span, stages = plan.n, plan.nx, plan.dl, plan.nch, plan.span, plan.stages
    return pl.pallas_call(
        functools.partial(body_kernel, plan),
        out_shape=jax.ShapeDtypeStruct((plan.tokens, dl), bf16),
        in_specs=[hbm, vmem, vmem, vmem, hbm, hbm, hbm],
        out_specs=vmem,
        scratch_shapes=[
            pltpu.VMEM((nch, 2 * LANES, dl), bf16),
            pltpu.VMEM((plan.layers, nch * LANES, dl), bf16),
            pltpu.VMEM((2, stages, span, 2, BLOCK, LANES), bf16),
            pltpu.VMEM((2, stages, span, BLOCK, LANES), bf16),
            pltpu.VMEM((2, span, 2, HALO, LANES), f32),
            pltpu.VMEM((plan.tokens, dl), f32),
            pltpu.VMEM((plan.layers + 1, plan.tokens, dl), bf16),
            pltpu.VMEM((plan.tokens, dl), bf16),
            pltpu.VMEM((plan.tokens, 1), f32),
            pltpu.VMEM((plan.half, dl), f32),
            pltpu.VMEM((plan.half, dl), bf16),
            pltpu.VMEM((stages, plan.half, dl), bf16),
            pltpu.VMEM((stages, nx, plan.half, dl), bf16),
            pltpu.VMEM((stages, n, 8, LANES), f32),
            pltpu.VMEM((stages, n, 8, LANES), f32),
            dma((plan.blocks,)),
            dma((2, nch)),
            dma((2,)),
            dma((plan.layers,)),
            dma((2, stages, span)),
            dma((2, stages, span)),
            dma((2, stages, span)),
            dma((2, stages, span)),
            dma((stages, n)),
            dma((stages, n)),
            dma((stages, n)),
            dma((stages, n)),
            dma((stages, nx)),
            dma((stages, nx)),
            dma((stages,)),
            dma((stages,)),
            dma((stages,)),
            dma((stages,)),
        ],
        compiler_params=pltpu.CompilerParams(
            collective_id=0, has_side_effects=True, vmem_limit_bytes=58 * 1024 * 1024
        ),
        name="sublayers",
    )(state, pre, post, coef, gate_weight, up_weight, down_weight)


def local(
    n,
    nx,
    tokens,
    pre_gain,
    post_gain,
    gate_weight,
    up_weight,
    gate_taps,
    up_taps,
    gate_bias,
    up_bias,
    down_weight,
):
    layers, dl, fl = gate_weight.shape
    plan = Plan(layers, n, nx, tokens.shape[0], dl, fl)
    padding = -fl % LANES
    coefs = jnp.concatenate(
        [gate_taps, gate_bias[:, None], up_taps, up_bias[:, None]], axis=1
    ).astype(jnp.float32)
    coefs = jnp.pad(coefs, ((0, 0), (0, 0), (0, padding)))
    pre, post = pre_gain.astype(jnp.float32), post_gain.astype(jnp.float32)
    gate_cols = jnp.swapaxes(gate_weight, 1, 2)
    up_cols = jnp.swapaxes(up_weight, 1, 2)
    return run(plan, tokens, pre, post, coefs, gate_cols, up_cols, down_weight)


def solution(mesh):
    in_specs = (
        P("grp", "ra"),
        P(None, "ra"),
        P(None, "ra"),
        P(None, "ra", "cb"),
        P(None, "ra", "cb"),
        P(None, None, "cb"),
        P(None, None, "cb"),
        P(None, "cb"),
        P(None, "cb"),
        P(None, "cb", "ra"),
    )
    body = functools.partial(local, mesh.shape["ra"], mesh.shape["cb"] // 2)
    return jax.shard_map(
        body, mesh=mesh, in_specs=in_specs, out_specs=P("grp", "ra"), check_vma=False
    )
```

```python
import functools

import jax
import jax.numpy as jnp
from jax import lax
from jax.experimental import pallas as pl
from jax.experimental.pallas import tpu as pltpu
from jax.sharding import PartitionSpec as P

LEN = 256
LANES = 128
BLOCK = 128
HALO = 8
SUM_SKEW = 3
HID_SKEW = 3

epsilon = 1e-06
residual_scale = 0.5
MESH = pl.DeviceIdType.MESH


class Plan:
    def __init__(self, layers, n, nx, tokens, dl, fl, taps):
        self.layers, self.n, self.nx = layers, n, nx
        self.tokens, self.dl, self.fl = tokens, dl, fl
        self.side = taps + 1
        self.nfull = fl // LANES
        self.nch = -(-fl // LANES)
        self.tail = fl - self.nfull * LANES
        self.packed = 0 < 2 * self.tail <= LANES
        self.blocks = tokens // BLOCK
        self.per_seq = LEN // BLOCK
        self.span = -(-self.nch // 2)
        self.half = BLOCK // 2
        self.stages = layers * self.blocks
        self.tiles = [
            layers * sum(self.tiles_of(d, b) for b in range(self.blocks)) for d in range(2)]
        self.hids = [
            layers * sum(len(self.chunks(d, b)) for b in range(self.blocks)) for d in range(2)]
        self.turn = (n - 1) * SUM_SKEW
        self.done = self.turn + (n - 1) * HID_SKEW
        self.pair_at = self.done + 2
        self.x_at = self.pair_at + 4
        self.norm_at = self.x_at + 3
        self.next_at = self.norm_at + 1
        self.period = max(
            self.blocks * self.span,
            self.span + self.next_at + 1,
            (self.blocks - 1) * self.span + self.turn + 2,
        )
        self.steps = (layers - 1) * self.period + self.blocks * self.span + self.next_at + 1

    def chunks(self, d, b):
        return range((d + b // self.per_seq) % 2, self.nch, 2)

    def tiles_of(self, d, b):
        chunks = self.chunks(d, b)
        return 2 * len(chunks) - (1 if self.packed and self.nfull in chunks else 0)


def body_kernel(
    plan,
    state_hbm, pre_ref, post_ref, gt_ref, ut_ref, gb_ref, ub_ref, wg_hbm, wu_hbm, wd_hbm,
    out_ref,
    gains, coefs, w, wd, part, hid, halo, acc, states, normed, scale, branch, pair_out, pair_in, xbuf, pre_sq, post_sq,
    ssem, wsem, wtail, wdsem, part_send, part_recv, hid_send, hid_recv,
    pre_send, pre_recv, post_send, post_recv, x_send, x_recv, pair_send, pair_recv,
    back_send, back_recv,
):
    z = lax.axis_index("ra")
    k = lax.axis_index("cb")
    core, xi = k % 2, k // 2
    peer = k + 1 - 2 * core
    n, nx, layers, dl, fl = plan.n, plan.nx, plan.layers, plan.dl, plan.fl
    nch, nfull, tail, blocks, span, half = (
        plan.nch, plan.nfull, plan.tail, plan.blocks, plan.span, plan.half)
    width = dl * n
    f32 = jnp.float32

    def w_copies(layer, c):
        cols = pl.ds(pl.multiple_of(c * LANES, LANES), LANES)
        return (
            pltpu.make_async_copy(
                wg_hbm.at[layer, cols], w.at[c, pl.ds(0, LANES)], wsem.at[0, c]),
            pltpu.make_async_copy(
                wu_hbm.at[layer, cols], w.at[c, pl.ds(LANES, LANES)], wsem.at[1, c]),
        )

    up_at = tail if plan.packed else LANES

    def tail_copies(layer):
        cols = pl.ds(nfull * LANES, tail)
        return (
            pltpu.make_async_copy(
                wg_hbm.at[layer, cols], w.at[nfull, pl.ds(0, tail)], wtail.at[0]),
            pltpu.make_async_copy(
                wu_hbm.at[layer, cols], w.at[nfull, pl.ds(up_at, tail)], wtail.at[1]),
        )

    def w_do(layer, c, act):
        @pl.when(c < nfull)
        def _():
            for copy in w_copies(layer, c):
                act(copy)

        if tail:
            @pl.when(c == nfull)
            def _():
                for copy in tail_copies(layer):
                    act(copy)

    def start(copy):
        copy.start()

    def wait(copy):
        copy.wait()

    def wd_copy(layer):
        return pltpu.make_async_copy(
            wd_hbm.at[layer], wd.at[layer, pl.ds(0, fl)], wdsem.at[layer])

    def block_rows(b):
        return pl.ds(pl.multiple_of(b * BLOCK, BLOCK), BLOCK)

    def half_rows(b, which):
        return pl.ds(pl.multiple_of(b * BLOCK + which * half, half), half)

    def state_rows(layer, b):
        return block_rows(layer * blocks + b)

    def state_half(layer, b, which):
        return half_rows(layer * blocks + b, which)

    def state_copy(b):
        return pltpu.make_async_copy(
            state_hbm.at[block_rows(b)], states.at[block_rows(b)], ssem.at[b])

    barrier = pltpu.get_barrier_semaphore()

    @pl.loop(1, n)
    def _(o):
        pl.semaphore_signal(
            barrier, inc=1, device_id={"ra": (z + o) % n}, device_id_type=MESH)

    pl.semaphore_signal(barrier, inc=1, device_id={"cb": peer}, device_id_type=MESH)
    for o in range(1, nx):
        pl.semaphore_signal(
            barrier, inc=1, device_id={"cb": (xi + o) % nx * 2 + core}, device_id_type=MESH)

    for b in range(blocks):
        state_copy(b).start()

    @pl.loop(0, nch)
    def _(c):
        w_do(0, c, start)

    for layer in range(layers):
        wd_copy(layer).start()

    def eye(rows):
        shape = (rows, LANES)
        return lax.broadcasted_iota(jnp.int32, shape, 0) == lax.broadcasted_iota(
            jnp.int32, shape, 1)

    def to_row(column):
        return jnp.sum(jnp.where(eye(column.shape[0]), column, 0.0), axis=0, keepdims=True)

    def to_column(row, rows):
        return jnp.sum(jnp.where(eye(rows), row, 0.0), axis=1, keepdims=True)

    def sq_copy(buf, send, recv, t, o, slot):
        return pltpu.make_async_remote_copy(
            src_ref=buf.at[t * n + slot], dst_ref=buf.at[t * n + slot],
            send_sem=send.at[0], recv_sem=recv.at[t, slot],
            device_id={"ra": (z + o) % n}, device_id_type=MESH)

    def sq_start(buf, send, recv, t):
        @pl.loop(1, n)
        def _(o):
            sq_copy(buf, send, recv, t, o, z).start()

    def sq_wait(buf, send, recv, t):
        @pl.loop(1, n)
        def _(o):
            sq_copy(buf, send, recv, t, o, (z + o) % n).wait_recv()

    def scale_of(buf, t, rows):
        total = buf[t * n, 0:1, :]
        for slot in range(1, n):
            total = total + buf[t * n + slot, 0:1, :]
        return to_column(lax.rsqrt(total / width + epsilon), rows)

    def norm(layer, b):
        t = layer * blocks + b
        wide = states[state_rows(layer, b), :].astype(f32)
        normed[block_rows(b), :] = (wide * gains[layer, 0:1, :]).astype(normed.dtype)
        row = to_row(jnp.sum(wide * wide, axis=1, keepdims=True))
        pre_sq[t * n + z] = jnp.broadcast_to(row, pre_sq.shape[1:])

    if tail:
        for lo, hi in ((tail, up_at), (up_at + tail, 2 * LANES)):
            if lo < hi:
                w[nfull, lo:hi, :] = jnp.zeros((hi - lo, dl), w.dtype)
        for layer in range(layers):
            wd[layer, fl:, :] = jnp.zeros((nch * LANES - fl, dl), wd.dtype)

    taps = gt_ref.shape[0]
    side = taps + 1
    for layer in range(layers):
        gains[layer, 0:1, :] = pre_ref[layer : layer + 1, :].astype(f32)
        gains[layer, 1:2, :] = post_ref[layer : layer + 1, :].astype(f32)
    state_copy(0).wait()
    norm(0, 0)
    pl.semaphore_wait(barrier, n - 1 + nx)
    sq_start(pre_sq, pre_send, pre_recv, 0)

    def fill_coefs():
        if tail:
            coefs[:, :, nfull * LANES :] = jnp.zeros((layers, coefs.shape[1], LANES), f32)
        for at, (tap_ref, bias_ref) in ((0, (gt_ref, gb_ref)), (side, (ut_ref, ub_ref))):
            for i in range(side):
                both = (tap_ref[i] if i < taps else bias_ref[...]).astype(f32)
                for layer in range(layers):
                    coefs[layer, at + i : at + i + 1, 0:fl] = both[layer : layer + 1, :]
        if plan.packed:
            last = slice(nfull * LANES, (nfull + 1) * LANES)
            for layer in range(layers):
                for i in range(side):
                    up = coefs[layer, side + i : side + i + 1, last]
                    coefs[layer, i : i + 1, last] += pltpu.roll(up, tail, 1)

    def place(d):
        if d == 0:
            return n - 1 - z, z - 1, z + 1
        return z, z + 1, z - 1

    def part_tile(t, j, i):
        return (t * span + j) * 2 + i

    def part_do(d, t, j, c, target, act):
        def go(count):
            tiles = pl.ds(part_tile(t, j, 0), count)
            act(pltpu.make_async_remote_copy(
                src_ref=part.at[d, tiles], dst_ref=part.at[d, tiles],
                send_sem=part_send.at[d], recv_sem=part_recv.at[d, t, j],
                device_id={"ra": target}, device_id_type=MESH))

        if plan.packed:
            @pl.when(c < nfull)
            def _():
                go(2)

            @pl.when(c == nfull)
            def _():
                go(1)
        else:
            go(2)

    def wait_recv(copy):
        copy.wait_recv()

    def hid_copy(d, t, j, target):
        return pltpu.make_async_remote_copy(
            src_ref=hid.at[d, t * span + j], dst_ref=hid.at[d, t * span + j],
            send_sem=hid_send.at[d], recv_sem=hid_recv.at[d, t, j],
            device_id={"ra": target}, device_id_type=MESH)

    def decode(g):
        live = g >= 0
        g = jnp.maximum(g, 0)
        layer = g // plan.period
        rest = g - layer * plan.period
        b = rest // span
        j = rest - b * span
        return live & (layer < layers) & (b < blocks), layer, b, j

    def chunk_of(d, b, j):
        return 2 * j + (d + b // plan.per_seq) % 2

    def conv(values, before, taps, bias):
        rows = lax.broadcasted_iota(jnp.int32, before.shape, 0)
        count = len(taps)
        result = taps[count - 1] * values
        for offset in range(1, count):
            moved = pltpu.roll(values, offset, 0)
            head = jnp.where(rows < offset, pltpu.roll(before, offset, 0), moved[:HALO])
            moved = jnp.concatenate([head, moved[HALO:]], axis=0)
            result = result + taps[count - 1 - offset] * moved
        return result + bias

    def wd_rows(c):
        return pl.ds(pl.multiple_of(c * LANES, LANES), LANES)

    def add_down(d, layer, b, j, c):
        at = (layer * blocks + b) * span + j

        @pl.when(j % 2 == 1)
        def _():
            two = jnp.concatenate([hid[d, at - 1], hid[d, at]], axis=1)
            rows = jnp.concatenate([wd[layer, wd_rows(c - 2), :], wd[layer, wd_rows(c), :]], axis=0)
            acc[block_rows(b), :] += jnp.dot(two, rows, preferred_element_type=f32)

        @pl.when((j % 2 == 0) & (c + 2 >= nch))
        def _():
            acc[block_rows(b), :] += jnp.dot(
                hid[d, at], wd[layer, wd_rows(c), :], preferred_element_type=f32)

    def pair_copy(t):
        return pltpu.make_async_remote_copy(
            src_ref=pair_out, dst_ref=pair_in.at[t],
            send_sem=pair_send.at[t], recv_sem=pair_recv.at[t],
            device_id={"cb": peer}, device_id_type=MESH)

    def x_copy(t, o, slot):
        return pltpu.make_async_remote_copy(
            src_ref=xbuf.at[t * nx + slot], dst_ref=xbuf.at[t * nx + slot],
            send_sem=x_send.at[0], recv_sem=x_recv.at[t, slot],
            device_id={"cb": (xi + o) % nx * 2 + core}, device_id_type=MESH)

    def back_copy(layer, b, which):
        rows = state_half(layer + 1, b, which)
        t = layer * blocks + b
        return pltpu.make_async_remote_copy(
            src_ref=states.at[rows], dst_ref=states.at[rows],
            send_sem=back_send.at[0], recv_sem=back_recv.at[t],
            device_id={"cb": peer}, device_id_type=MESH)

    @pl.loop(0, plan.steps)
    def _(s):
        @pl.when(s == 2)
        def _():
            fill_coefs()

        @pl.when((s >= 1) & (s < blocks))
        def _():
            state_copy(s).wait()
            norm(0, s)
            sq_start(pre_sq, pre_send, pre_recv, s)

        live, layer, b, j = decode(s - plan.turn)

        @pl.when(live & (j == 0))
        def _():
            t = layer * blocks + b

            @pl.when(b == 0)
            def _():
                wd_copy(layer).wait()

            sq_wait(pre_sq, pre_send, pre_recv, t)
            scale[block_rows(b), :] = scale_of(pre_sq, t, BLOCK)
            acc[block_rows(b), :] = jnp.zeros((BLOCK, dl), f32)

        for d in range(2):
            p, nxt, prv = place(d)
            live, layer, b, j = decode(s - p * SUM_SKEW)
            c = chunk_of(d, b, j)
            t = layer * blocks + b

            @pl.when(live & (c < nch))
            def _():
                @pl.when(b == 0)
                def _():
                    w_do(layer, c, wait)

                own = lax.dot_general(
                    normed[block_rows(b), :], w[c], (((1,), (1,)), ((), ())),
                    preferred_element_type=f32)

                def mine(i):
                    return own[:, i * LANES : (i + 1) * LANES]

                def tile(i):
                    return part[d, part_tile(t, j, i)].astype(f32)

                @pl.when(p == 0)
                def _():
                    for i in range(2):
                        part[d, part_tile(t, j, i)] = mine(i).astype(part.dtype)
                    part_do(d, t, j, c, nxt, start)

                @pl.when((p > 0) & (p < n - 1))
                def _():
                    part_do(d, t, j, c, nxt, wait_recv)
                    part[d, part_tile(t, j, 0)] = (tile(0) + mine(0)).astype(part.dtype)

                    @pl.when((c < nfull) | (not plan.packed))
                    def _():
                        part[d, part_tile(t, j, 1)] = (tile(1) + mine(1)).astype(part.dtype)

                    part_do(d, t, j, c, nxt, start)

                @pl.when(p == n - 1)
                def _():
                    part_do(d, t, j, c, prv, wait_recv)
                    coef = coefs[layer, :, wd_rows(c)]
                    row = [coef[i : i + 1, :] for i in range(2 * side)]
                    first = b % plan.per_seq == 0
                    last = plan.packed & (c == nfull)
                    sides = []
                    for i in range(2):
                        arrived = jnp.where(last, 0.0, tile(i)) if i and plan.packed else tile(i)
                        total = (arrived + mine(i)) * scale[block_rows(b), :]
                        before = jnp.where(first, 0.0, halo[d, j, i])
                        halo[d, j, i] = total[BLOCK - HALO :, :]
                        at = i * side
                        sides.append(conv(total, before, row[at : at + taps], row[at + taps]))
                    gate, up = sides
                    if plan.packed:
                        up = jnp.where(last, pltpu.roll(gate, LANES - tail, 1), up)
                    value = jax.nn.gelu(gate, approximate=True) * up
                    if plan.packed:
                        lane = lax.broadcasted_iota(jnp.int32, value.shape, 1)
                        value = jnp.where(last & (lane >= tail), 0.0, value)
                    hid[d, t * span + j] = value.astype(hid.dtype)
                    hid_copy(d, t, j, prv).start()

                @pl.when((b == blocks - 1) & (layer + 1 < layers))
                def _():
                    w_do(layer + 1, c, start)

        for d in range(2):
            p, nxt, prv = place(d)
            live, layer, b, j = decode(s - (plan.done - p * HID_SKEW))
            c = chunk_of(d, b, j)
            t = layer * blocks + b

            @pl.when(live & (p < n - 1) & (c < nch))
            def _():
                hid_copy(d, t, j, nxt).wait_recv()

                @pl.when(p > 0)
                def _():
                    hid_copy(d, t, j, prv).start()

        for d in range(2):
            p, nxt, prv = place(d)
            live, layer, b, j = decode(s - (plan.done - p * HID_SKEW))
            c = chunk_of(d, b, j)

            @pl.when(live & (c < nch))
            def _():
                add_down(d, layer, b, j, c)

        live, layer, b, j = decode(s - plan.done)

        @pl.when(live & (j == span - 1))
        def _():
            t = layer * blocks + b
            pair_out[...] = acc[half_rows(b, 1 - core), :].astype(pair_out.dtype)
            pair_copy(t).start()

        live, layer, b, j = decode(s - plan.pair_at)

        @pl.when(live & (j == span - 1))
        def _():
            t = layer * blocks + b
            pair_copy(t).wait()
            xbuf[t * nx + xi] = (
                acc[half_rows(b, core), :] + pair_in[t].astype(f32)).astype(xbuf.dtype)
            for o in range(1, nx):
                x_copy(t, o, xi).start()

        live, layer, b, j = decode(s - plan.x_at)

        @pl.when(live & (j == span - 1))
        def _():
            t = layer * blocks + b
            for o in range(1, nx):
                x_copy(t, o, (xi + o) % nx).wait_recv()
            total = xbuf[t * nx].astype(f32)
            for i in range(1, nx):
                total = total + xbuf[t * nx + i].astype(f32)
            branch[...] = total
            row = to_row(jnp.sum(total * total, axis=1, keepdims=True))
            post_sq[t * n + z] = jnp.broadcast_to(row, post_sq.shape[1:])
            sq_start(post_sq, post_send, post_recv, t)

        live, layer, b, j = decode(s - plan.norm_at)

        @pl.when(live & (j == span - 1))
        def _():
            t = layer * blocks + b
            sq_wait(post_sq, post_send, post_recv, t)
            states[state_half(layer + 1, b, core), :] = (
                residual_scale * states[state_half(layer, b, core), :].astype(f32)
                + branch[...] * scale_of(post_sq, t, half) * gains[layer, 1:2, :]
            ).astype(states.dtype)
            back_copy(layer, b, core).start()

        live, layer, b, j = decode(s - plan.next_at)

        @pl.when(live & (j == span - 1))
        def _():
            t = layer * blocks + b
            back_copy(layer, b, 1 - core).wait_recv()

            @pl.when(layer + 1 < layers)
            def _():
                norm(layer + 1, b)
                sq_start(pre_sq, pre_send, pre_recv, t + blocks)

            @pl.when(layer + 1 == layers)
            def _():
                out_ref[block_rows(b), :] = states[state_rows(layers, b), :]

    def all_sent(buf, count, sem):
        sent = buf.at[pl.ds(0, count)]
        pltpu.make_async_remote_copy(
            src_ref=sent, dst_ref=sent, send_sem=sem, recv_sem=pair_recv.at[0],
            device_id={"cb": peer}, device_id_type=MESH).wait_send()

    all_sent(states, plan.stages * half, back_send.at[0])
    if nx > 1:
        all_sent(xbuf, plan.stages * (nx - 1), x_send.at[0])
    all_sent(pre_sq, plan.stages * (n - 1), pre_send.at[0])
    all_sent(post_sq, plan.stages * (n - 1), post_send.at[0])
    for d in range(2):
        p, nxt, prv = place(d)

        @pl.when(p < n - 1)
        def _():
            all_sent(part.at[d], plan.tiles[d], part_send.at[d])

        @pl.when(p > 0)
        def _():
            all_sent(hid.at[d], plan.hids[d], hid_send.at[d])


def run(plan, *operands):
    vmem = pl.BlockSpec(memory_space=pltpu.VMEM)
    hbm = pl.BlockSpec(memory_space=pl.ANY)
    dma = pltpu.SemaphoreType.DMA
    bf16, f32 = jnp.bfloat16, jnp.float32
    n, nx, dl, nch, span, stages = plan.n, plan.nx, plan.dl, plan.nch, plan.span, plan.stages
    return pl.pallas_call(
        functools.partial(body_kernel, plan),
        out_shape=jax.ShapeDtypeStruct((plan.tokens, dl), bf16),
        in_specs=[hbm] + [vmem] * 6 + [hbm] * 3,
        out_specs=vmem,
        scratch_shapes=[
            pltpu.VMEM((plan.layers, 2, dl), f32),
            pltpu.VMEM((plan.layers, 2 * plan.side, nch * LANES), f32),
            pltpu.VMEM((nch, 2 * LANES, dl), bf16),
            pltpu.VMEM((plan.layers, nch * LANES, dl), bf16),
            pltpu.VMEM((2, stages * span * 2, BLOCK, LANES), bf16),
            pltpu.VMEM((2, stages * span, BLOCK, LANES), bf16),
            pltpu.VMEM((2, span, 2, HALO, LANES), f32),
            pltpu.VMEM((plan.tokens, dl), f32),
            pltpu.VMEM(((plan.layers + 1) * plan.tokens, dl), bf16),
            pltpu.VMEM((plan.tokens, dl), bf16),
            pltpu.VMEM((plan.tokens, 1), f32),
            pltpu.VMEM((plan.half, dl), f32),
            pltpu.VMEM((plan.half, dl), bf16),
            pltpu.VMEM((stages, plan.half, dl), bf16),
            pltpu.VMEM((stages * nx, plan.half, dl), bf16),
            pltpu.VMEM((stages * n, 8, LANES), f32),
            pltpu.VMEM((stages * n, 8, LANES), f32),
            dma((plan.blocks,)),
            dma((2, nch)),
            dma((2,)),
            dma((plan.layers,)),
            dma((2,)),
            dma((2, stages, span)),
            dma((2,)),
            dma((2, stages, span)),
            dma((1,)),
            dma((stages, n)),
            dma((1,)),
            dma((stages, n)),
            dma((1,)),
            dma((stages, nx)),
            dma((stages,)),
            dma((stages,)),
            dma((1,)),
            dma((stages,)),
        ],
        compiler_params=pltpu.CompilerParams(
            collective_id=0, has_side_effects=True, vmem_limit_bytes=58 * 1024 * 1024
        ),
        name="sublayers",
    )(*operands)


def local(
    n,
    nx,
    tokens,
    pre_gain,
    post_gain,
    gate_weight,
    up_weight,
    gate_taps,
    up_taps,
    gate_bias,
    up_bias,
    down_weight,
):
    layers, dl, fl = gate_weight.shape
    plan = Plan(layers, n, nx, tokens.shape[0], dl, fl, gate_taps.shape[1])
    return run(
        plan, tokens, pre_gain, post_gain, jnp.swapaxes(gate_taps, 0, 1), jnp.swapaxes(up_taps, 0, 1),
        gate_bias, up_bias, jnp.swapaxes(gate_weight, 1, 2), jnp.swapaxes(up_weight, 1, 2), down_weight)


def solution(mesh):
    in_specs = (
        P("grp", "ra"),
        P(None, "ra"),
        P(None, "ra"),
        P(None, "ra", "cb"),
        P(None, "ra", "cb"),
        P(None, None, "cb"),
        P(None, None, "cb"),
        P(None, "cb"),
        P(None, "cb"),
        P(None, "cb", "ra"),
    )
    body = functools.partial(local, mesh.shape["ra"], mesh.shape["cb"] // 2)
    return jax.shard_map(
        body, mesh=mesh, in_specs=in_specs, out_specs=P("grp", "ra"), check_vma=False
    )
```

```python
import functools

import jax
import jax.numpy as jnp
from jax import lax
from jax.experimental import pallas as pl
from jax.experimental.pallas import tpu as pltpu
from jax.sharding import PartitionSpec as P

LEN = 256
LANES = 128
BLOCK = 128
HALO = 8
SUM_SKEW = 3
HID_SKEW = 3
LAST = 3

epsilon = 1e-06
residual_scale = 0.5
MESH = pl.DeviceIdType.MESH


class Plan:
    def __init__(self, layers, n, nx, tokens, dl, fl, taps):
        self.layers, self.n, self.nx = layers, n, nx
        self.tokens, self.dl, self.fl = tokens, dl, fl
        self.side = taps + 1
        self.nfull = fl // LANES
        self.nch = -(-fl // LANES)
        self.tail = fl - self.nfull * LANES
        self.packed = 0 < 2 * self.tail <= LANES
        self.blocks = tokens // BLOCK
        self.per_seq = LEN // BLOCK
        self.span = -(-self.nch // 2)
        self.half = BLOCK // 2
        self.stages = layers * self.blocks
        self.tiles = [
            layers * sum(self.tiles_of(d, b) for b in range(self.blocks)) for d in range(2)]
        self.lasts = [
            sum(c // 2 >= self.span - LAST for c in self.chunks(d, self.blocks - 1)) for d in range(2)]
        self.hids = [
            layers * sum(len(self.chunks(d, b)) for b in range(self.blocks)) - self.lasts[d]
            for d in range(2)]
        self.turn = (n - 1) * SUM_SKEW
        self.done = self.turn + (n - 1) * HID_SKEW
        self.pair_at = self.done + 2
        self.x_at = self.pair_at + 8
        self.norm_at = self.x_at + 3
        self.next_at = self.norm_at + 1
        least = max(self.span + self.next_at + 1, (self.blocks - 1) * self.span + self.turn + 2)
        self.lap = max(self.blocks, -(-least // self.span))
        self.steps = ((layers - 1) * self.lap + self.blocks) * self.span + self.next_at + 1
        self.ring = -(-(SUM_SKEW + HID_SKEW + 2) // self.span)

    def chunks(self, d, b):
        return range((d + b // self.per_seq) % 2, self.nch, 2)

    def tiles_of(self, d, b):
        chunks = self.chunks(d, b)
        return 2 * len(chunks) - (1 if self.packed and self.nfull in chunks else 0)


def body_kernel(
    plan,
    state_hbm, pre_ref, post_ref, gt_ref, ut_ref, gb_ref, ub_ref, wg_hbm, wu_hbm, wd_hbm,
    out_ref,
    gains, coefs, w, wd, part, hid, halo, acc, states, normed, scale, branch, pair_out, pair_in, xbuf, pre_sq, post_sq,
    ssem, wsem, wtail, wdsem, part_send, part_recv, hid_send, hid_recv, last_recv,
    pre_send, pre_recv, post_send, post_recv, x_send, x_recv, pair_send, pair_recv,
    back_send, back_recv,
):
    z = lax.axis_index("ra")
    k = lax.axis_index("cb")
    core, xi = k % 2, k // 2
    peer = k + 1 - 2 * core
    n, nx, layers, dl, fl = plan.n, plan.nx, plan.layers, plan.dl, plan.fl
    nch, nfull, tail, blocks, span, half = (
        plan.nch, plan.nfull, plan.tail, plan.blocks, plan.span, plan.half)
    width = dl * n
    f32 = jnp.float32

    def w_copies(layer, c):
        cols = pl.ds(pl.multiple_of(c * LANES, LANES), LANES)
        return (
            pltpu.make_async_copy(
                wg_hbm.at[layer, cols], w.at[c, pl.ds(0, LANES)], wsem.at[0, c]),
            pltpu.make_async_copy(
                wu_hbm.at[layer, cols], w.at[c, pl.ds(LANES, LANES)], wsem.at[1, c]),
        )

    up_at = tail if plan.packed else LANES

    def tail_copies(layer):
        cols = pl.ds(nfull * LANES, tail)
        return (
            pltpu.make_async_copy(
                wg_hbm.at[layer, cols], w.at[nfull, pl.ds(0, tail)], wtail.at[0]),
            pltpu.make_async_copy(
                wu_hbm.at[layer, cols], w.at[nfull, pl.ds(up_at, tail)], wtail.at[1]),
        )

    def w_do(layer, c, act):
        @pl.when(c < nfull)
        def _():
            for copy in w_copies(layer, c):
                act(copy)

        if tail:
            @pl.when(c == nfull)
            def _():
                for copy in tail_copies(layer):
                    act(copy)

    def start(copy):
        copy.start()

    def wait(copy):
        copy.wait()

    def wd_copy(layer):
        return pltpu.make_async_copy(
            wd_hbm.at[layer], wd.at[layer, pl.ds(0, fl)], wdsem.at[layer])

    def block_rows(b):
        return pl.ds(pl.multiple_of(b * BLOCK, BLOCK), BLOCK)

    def half_rows(b, which):
        return pl.ds(pl.multiple_of(b * BLOCK + which * half, half), half)

    def state_rows(layer, b):
        return block_rows(layer * blocks + b)

    def state_half(layer, b, which):
        return half_rows(layer * blocks + b, which)

    def state_copy(b):
        return pltpu.make_async_copy(
            state_hbm.at[block_rows(b)], states.at[block_rows(b)], ssem.at[b])

    barrier = pltpu.get_barrier_semaphore()

    @pl.loop(1, n)
    def _(o):
        pl.semaphore_signal(
            barrier, inc=1, device_id={"ra": (z + o) % n}, device_id_type=MESH)

    pl.semaphore_signal(barrier, inc=1, device_id={"cb": peer}, device_id_type=MESH)
    for o in range(1, nx):
        pl.semaphore_signal(
            barrier, inc=1, device_id={"cb": (xi + o) % nx * 2 + core}, device_id_type=MESH)

    for b in range(blocks):
        state_copy(b).start()

    @pl.loop(0, nch)
    def _(c):
        w_do(0, c, start)

    for layer in range(layers):
        wd_copy(layer).start()

    def eye(rows):
        shape = (rows, LANES)
        return lax.broadcasted_iota(jnp.int32, shape, 0) == lax.broadcasted_iota(
            jnp.int32, shape, 1)

    def to_row(column):
        return jnp.sum(jnp.where(eye(column.shape[0]), column, 0.0), axis=0, keepdims=True)

    def to_column(row, rows):
        return jnp.sum(jnp.where(eye(rows), row, 0.0), axis=1, keepdims=True)

    def sq_copy(buf, send, recv, t, o, slot):
        return pltpu.make_async_remote_copy(
            src_ref=buf.at[t * n + slot], dst_ref=buf.at[t * n + slot],
            send_sem=send.at[0], recv_sem=recv.at[t % blocks, slot],
            device_id={"ra": (z + o) % n}, device_id_type=MESH)

    def sq_start(buf, send, recv, t):
        @pl.loop(1, n)
        def _(o):
            sq_copy(buf, send, recv, t, o, z).start()

    def sq_wait(buf, send, recv, t):
        @pl.loop(1, n)
        def _(o):
            sq_copy(buf, send, recv, t, o, (z + o) % n).wait_recv()

    def scale_of(buf, t, rows):
        total = buf[t * n, 0:1, :]
        for slot in range(1, n):
            total = total + buf[t * n + slot, 0:1, :]
        return to_column(lax.rsqrt(total / width + epsilon), rows)

    def norm(layer, b):
        t = layer * blocks + b
        wide = states[state_rows(layer, b), :].astype(f32)
        normed[block_rows(b), :] = (wide * gains[layer, 0:1, :]).astype(normed.dtype)
        row = to_row(jnp.sum(wide * wide, axis=1, keepdims=True))
        pre_sq[t * n + z] = jnp.broadcast_to(row, pre_sq.shape[1:])

    if tail:
        for lo, hi in ((tail, up_at), (up_at + tail, 2 * LANES)):
            if lo < hi:
                w[nfull, lo:hi, :] = jnp.zeros((hi - lo, dl), w.dtype)
        for layer in range(layers):
            wd[layer, fl:, :] = jnp.zeros((nch * LANES - fl, dl), wd.dtype)

    taps = gt_ref.shape[0]
    side = taps + 1
    for layer in range(layers):
        gains[layer, 0:1, :] = pre_ref[layer : layer + 1, :].astype(f32)
        gains[layer, 1:2, :] = post_ref[layer : layer + 1, :].astype(f32)
    state_copy(0).wait()
    norm(0, 0)
    pl.semaphore_wait(barrier, n - 1 + nx)
    sq_start(pre_sq, pre_send, pre_recv, 0)

    def fill_coefs():
        if tail:
            coefs[:, :, nfull * LANES :] = jnp.zeros((layers, coefs.shape[1], LANES), f32)
        for at, (tap_ref, bias_ref) in ((0, (gt_ref, gb_ref)), (side, (ut_ref, ub_ref))):
            for i in range(side):
                both = (tap_ref[i] if i < taps else bias_ref[...]).astype(f32)
                for layer in range(layers):
                    coefs[layer, at + i : at + i + 1, 0:fl] = both[layer : layer + 1, :]
        if plan.packed:
            last = slice(nfull * LANES, (nfull + 1) * LANES)
            for layer in range(layers):
                for i in range(side):
                    up = coefs[layer, side + i : side + i + 1, last]
                    coefs[layer, i : i + 1, last] += pltpu.roll(up, tail, 1)

    def place(d):
        if d == 0:
            return n - 1 - z, z - 1, z + 1
        return z, z + 1, z - 1

    def part_tile(t, j, i):
        return (t * span + j) * 2 + i

    def part_do(d, t, j, c, target, act):
        def go(count):
            tiles = pl.ds(part_tile(t, j, 0), count)
            act(pltpu.make_async_remote_copy(
                src_ref=part.at[d, tiles], dst_ref=part.at[d, tiles],
                send_sem=part_send.at[d], recv_sem=part_recv.at[d, slot_of(t, j)],
                device_id={"ra": target}, device_id_type=MESH))

        if plan.packed:
            @pl.when(c < nfull)
            def _():
                go(2)

            @pl.when(c == nfull)
            def _():
                go(1)
        else:
            go(2)

    def wait_recv(copy):
        copy.wait_recv()

    def hid_copy(d, t, j, target):
        return pltpu.make_async_remote_copy(
            src_ref=hid.at[d, t * span + j], dst_ref=hid.at[d, t * span + j],
            send_sem=hid_send.at[d], recv_sem=hid_recv.at[d, slot_of(t, j)],
            device_id={"ra": target}, device_id_type=MESH)

    def last_copy(d, t, j, target):
        return pltpu.make_async_remote_copy(
            src_ref=hid.at[d, t * span + j], dst_ref=hid.at[d, t * span + j],
            send_sem=hid_send.at[d], recv_sem=last_recv.at[d, j - (span - LAST)],
            device_id={"ra": target}, device_id_type=MESH)

    def is_last(layer, b, j):
        return (layer == layers - 1) & (b == blocks - 1) & (j >= span - LAST)

    def one_of(b, members):
        return functools.reduce(jnp.logical_or, [b == i for i in members], jnp.bool_(False))

    def odd(b):
        return one_of(b, [i for i in range(blocks) if i // plan.per_seq % 2])

    def chunk_of(d, b, j):
        return 2 * j + jnp.where(odd(b), 1 - d, d)

    def slot_of(t, j):
        return j if plan.ring == 1 else t % plan.ring * span + j

    def advance(at, moving):
        layer, b, j = at
        j = j + jnp.where(moving, 1, 0)
        turn = j == span
        b = b + jnp.where(turn, 1, 0)
        lap = b == plan.lap
        return (
            layer + jnp.where(lap, 1, 0), jnp.where(lap, 0, b), jnp.where(turn, 0, j))

    def live_at(at, offset, s):
        layer, b, j = at
        live = (s >= offset) & (layer < layers)
        return live if plan.lap == blocks else live & (b < blocks)

    def ago(at, steps):
        layer, b, j = at
        laps = -(-steps // span)
        b = b - laps
        over = b < 0
        layer = jnp.where(over, layer - 1, layer)
        b = jnp.where(over, b + plan.lap, b)
        hit = (j == (span - 1 + steps) % span) & (layer >= 0) & (layer < layers)
        return hit if plan.lap == blocks else hit & (b < blocks), layer, b

    def conv(values, before, taps, bias):
        rows = lax.broadcasted_iota(jnp.int32, before.shape, 0)
        count = len(taps)
        result = taps[count - 1] * values
        for offset in range(1, count):
            moved = pltpu.roll(values, offset, 0)
            head = jnp.where(rows < offset, pltpu.roll(before, offset, 0), moved[:HALO])
            moved = jnp.concatenate([head, moved[HALO:]], axis=0)
            result = result + taps[count - 1 - offset] * moved
        return result + bias

    def wd_rows(c):
        return pl.ds(pl.multiple_of(c * LANES, LANES), LANES)

    def add_down(d, layer, b, j, c):
        at = (layer * blocks + b) * span + j

        @pl.when(j % 2 == 1)
        def _():
            two = jnp.concatenate([hid[d, at - 1], hid[d, at]], axis=1)
            rows = jnp.concatenate([wd[layer, wd_rows(c - 2), :], wd[layer, wd_rows(c), :]], axis=0)
            acc[block_rows(b), :] += jnp.dot(two, rows, preferred_element_type=f32)

        @pl.when((j % 2 == 0) & (c + 2 >= nch))
        def _():
            acc[block_rows(b), :] += jnp.dot(
                hid[d, at], wd[layer, wd_rows(c), :], preferred_element_type=f32)

    def pair_copy(t):
        return pltpu.make_async_remote_copy(
            src_ref=pair_out, dst_ref=pair_in.at[t],
            send_sem=pair_send.at[t % 2], recv_sem=pair_recv.at[t % 2],
            device_id={"cb": peer}, device_id_type=MESH)

    def x_copy(t, o, slot):
        return pltpu.make_async_remote_copy(
            src_ref=xbuf.at[t * nx + slot], dst_ref=xbuf.at[t * nx + slot],
            send_sem=x_send.at[0], recv_sem=x_recv.at[t % 2, slot],
            device_id={"cb": (xi + o) % nx * 2 + core}, device_id_type=MESH)

    def back_copy(layer, b, which):
        rows = state_half(layer + 1, b, which)
        t = layer * blocks + b
        return pltpu.make_async_remote_copy(
            src_ref=states.at[rows], dst_ref=states.at[rows],
            send_sem=back_send.at[0], recv_sem=back_recv.at[t % 2],
            device_id={"cb": peer}, device_id_type=MESH)

    offsets = [plan.turn, plan.done]
    for d in range(2):
        p = place(d)[0]
        offsets += [p * SUM_SKEW, plan.done - p * HID_SKEW]

    def step(s, streams):
        turn_at, done_at = streams[0], streams[1]
        sum_at, hid_at = streams[2::2], streams[3::2]

        @pl.when(s == 2)
        def _():
            fill_coefs()

        @pl.when((s >= 1) & (s < blocks))
        def _():
            state_copy(s).wait()
            norm(0, s)
            sq_start(pre_sq, pre_send, pre_recv, s)

        layer, b, j = turn_at

        @pl.when(live_at(turn_at, plan.turn, s) & (j == 0))
        def _():
            t = layer * blocks + b

            @pl.when(b == 0)
            def _():
                wd_copy(layer).wait()

            sq_wait(pre_sq, pre_send, pre_recv, t)
            scale[block_rows(b), :] = scale_of(pre_sq, t, BLOCK)
            acc[block_rows(b), :] = jnp.zeros((BLOCK, dl), f32)

        for d in range(2):
            p, nxt, prv = place(d)
            layer, b, j = sum_at[d]
            live = live_at(sum_at[d], p * SUM_SKEW, s)
            c = chunk_of(d, b, j)
            t = layer * blocks + b

            @pl.when(live & (c < nch))
            def _():
                @pl.when(b == 0)
                def _():
                    w_do(layer, c, wait)

                own = lax.dot_general(
                    normed[block_rows(b), :], w[c], (((1,), (1,)), ((), ())),
                    preferred_element_type=f32)

                def mine(i):
                    return own[:, i * LANES : (i + 1) * LANES]

                def tile(i):
                    return part[d, part_tile(t, j, i)].astype(f32)

                @pl.when(p == 0)
                def _():
                    for i in range(2):
                        part[d, part_tile(t, j, i)] = mine(i).astype(part.dtype)
                    part_do(d, t, j, c, nxt, start)

                @pl.when((p > 0) & (p < n - 1))
                def _():
                    part_do(d, t, j, c, nxt, wait_recv)
                    part[d, part_tile(t, j, 0)] = (tile(0) + mine(0)).astype(part.dtype)

                    @pl.when((c < nfull) | (not plan.packed))
                    def _():
                        part[d, part_tile(t, j, 1)] = (tile(1) + mine(1)).astype(part.dtype)

                    part_do(d, t, j, c, nxt, start)

                @pl.when(p == n - 1)
                def _():
                    part_do(d, t, j, c, prv, wait_recv)
                    coef = coefs[layer, :, wd_rows(c)]
                    row = [coef[i : i + 1, :] for i in range(2 * side)]
                    first = one_of(b, range(0, blocks, plan.per_seq))
                    last = plan.packed & (c == nfull)
                    sides = []
                    for i in range(2):
                        arrived = jnp.where(last, 0.0, tile(i)) if i and plan.packed else tile(i)
                        total = (arrived + mine(i)) * scale[block_rows(b), :]
                        before = jnp.where(first, 0.0, halo[d, j, i])
                        halo[d, j, i] = total[BLOCK - HALO :, :]
                        at = i * side
                        sides.append(conv(total, before, row[at : at + taps], row[at + taps]))
                    gate, up = sides
                    if plan.packed:
                        up = jnp.where(last, pltpu.roll(gate, LANES - tail, 1), up)
                    value = jax.nn.gelu(gate, approximate=True) * up
                    if plan.packed:
                        lane = lax.broadcasted_iota(jnp.int32, value.shape, 1)
                        value = jnp.where(last & (lane >= tail), 0.0, value)
                    hid[d, t * span + j] = value.astype(hid.dtype)

                    @pl.when(jnp.logical_not(is_last(layer, b, j)))
                    def _():
                        hid_copy(d, t, j, prv).start()

                    @pl.when(is_last(layer, b, j))
                    def _():
                        for o in range(n - 1, 0, -1):
                            last_copy(d, t, j, z + o * (prv - z)).start()

                @pl.when((b == blocks - 1) & (layer + 1 < layers))
                def _():
                    w_do(layer + 1, c, start)

        for d in range(2):
            p, nxt, prv = place(d)
            layer, b, j = hid_at[d]
            live = live_at(hid_at[d], plan.done - p * HID_SKEW, s)
            c = chunk_of(d, b, j)
            t = layer * blocks + b

            @pl.when(live & (p < n - 1) & (c < nch))
            def _():
                @pl.when(jnp.logical_not(is_last(layer, b, j)))
                def _():
                    hid_copy(d, t, j, nxt).wait_recv()

                    @pl.when(p > 0)
                    def _():
                        hid_copy(d, t, j, prv).start()

                @pl.when(is_last(layer, b, j))
                def _():
                    last_copy(d, t, j, nxt).wait_recv()

        for d in range(2):
            p, nxt, prv = place(d)
            layer, b, j = hid_at[d]
            live = live_at(hid_at[d], plan.done - p * HID_SKEW, s)
            c = chunk_of(d, b, j)

            @pl.when(live & (c < nch))
            def _():
                add_down(d, layer, b, j, c)

        started = s >= plan.done
        hit, layer, b = ago(done_at, 0)

        @pl.when(started & hit)
        def _():
            t = layer * blocks + b
            pair_out[...] = acc[half_rows(b, 1 - core), :].astype(pair_out.dtype)
            pair_copy(t).start()

        hit, layer, b = ago(done_at, plan.pair_at - plan.done)

        @pl.when(started & hit)
        def _():
            t = layer * blocks + b
            pair_copy(t).wait()
            xbuf[t * nx + xi] = (
                acc[half_rows(b, core), :] + pair_in[t].astype(f32)).astype(xbuf.dtype)
            for o in range(1, nx):
                x_copy(t, o, xi).start()

        hit, layer, b = ago(done_at, plan.x_at - plan.done)

        @pl.when(started & hit)
        def _():
            t = layer * blocks + b
            for o in range(1, nx):
                x_copy(t, o, (xi + o) % nx).wait_recv()
            total = xbuf[t * nx].astype(f32)
            for i in range(1, nx):
                total = total + xbuf[t * nx + i].astype(f32)
            branch[...] = total
            row = to_row(jnp.sum(total * total, axis=1, keepdims=True))
            post_sq[t * n + z] = jnp.broadcast_to(row, post_sq.shape[1:])
            sq_start(post_sq, post_send, post_recv, t)

        hit, layer, b = ago(done_at, plan.norm_at - plan.done)

        @pl.when(started & hit)
        def _():
            t = layer * blocks + b
            sq_wait(post_sq, post_send, post_recv, t)
            states[state_half(layer + 1, b, core), :] = (
                residual_scale * states[state_half(layer, b, core), :].astype(f32)
                + branch[...] * scale_of(post_sq, t, half) * gains[layer, 1:2, :]
            ).astype(states.dtype)
            back_copy(layer, b, core).start()

        hit, layer, b = ago(done_at, plan.next_at - plan.done)

        @pl.when(started & hit)
        def _():
            t = layer * blocks + b
            back_copy(layer, b, 1 - core).wait_recv()

            @pl.when(layer + 1 < layers)
            def _():
                norm(layer + 1, b)
                sq_start(pre_sq, pre_send, pre_recv, t + blocks)

            @pl.when(layer + 1 == layers)
            def _():
                out_ref[block_rows(b), :] = states[state_rows(layers, b), :]

        return tuple(
            advance(at, s >= offset) for at, offset in zip(streams, offsets, strict=True))

    lax.fori_loop(0, plan.steps, step, tuple((jnp.int32(0),) * 3 for _ in offsets))

    def all_sent(buf, count, sem):
        sent = buf.at[pl.ds(0, count)]
        pltpu.make_async_remote_copy(
            src_ref=sent, dst_ref=sent, send_sem=sem, recv_sem=pair_recv.at[0],
            device_id={"cb": peer}, device_id_type=MESH).wait_send()

    all_sent(states, plan.stages * half, back_send.at[0])
    if nx > 1:
        all_sent(xbuf, plan.stages * (nx - 1), x_send.at[0])
    all_sent(pre_sq, plan.stages * (n - 1), pre_send.at[0])
    all_sent(post_sq, plan.stages * (n - 1), post_send.at[0])
    for d in range(2):
        p, nxt, prv = place(d)

        @pl.when(p < n - 1)
        def _():
            all_sent(part.at[d], plan.tiles[d], part_send.at[d])

        @pl.when(p > 0)
        def _():
            all_sent(hid.at[d], plan.hids[d], hid_send.at[d])

        @pl.when(p == n - 1)
        def _():
            for o in range(1, n):
                all_sent(hid.at[d], plan.lasts[d], hid_send.at[d])


def run(plan, *operands):
    vmem = pl.BlockSpec(memory_space=pltpu.VMEM)
    hbm = pl.BlockSpec(memory_space=pl.ANY)
    dma = pltpu.SemaphoreType.DMA
    bf16, f32 = jnp.bfloat16, jnp.float32
    n, nx, dl, nch, span, stages = plan.n, plan.nx, plan.dl, plan.nch, plan.span, plan.stages
    return pl.pallas_call(
        functools.partial(body_kernel, plan),
        out_shape=pltpu.VMEM((plan.tokens, dl), bf16),
        in_specs=[hbm] + [vmem] * 6 + [hbm] * 3,
        out_specs=vmem,
        scratch_shapes=[
            pltpu.VMEM((plan.layers, 2, dl), f32),
            pltpu.VMEM((plan.layers, 2 * plan.side, nch * LANES), f32),
            pltpu.VMEM((nch, 2 * LANES, dl), bf16),
            pltpu.VMEM((plan.layers, nch * LANES, dl), bf16),
            pltpu.VMEM((2, stages * span * 2, BLOCK, LANES), bf16),
            pltpu.VMEM((2, stages * span, BLOCK, LANES), bf16),
            pltpu.VMEM((2, span, 2, HALO, LANES), f32),
            pltpu.VMEM((plan.tokens, dl), f32),
            pltpu.VMEM(((plan.layers + 1) * plan.tokens, dl), bf16),
            pltpu.VMEM((plan.tokens, dl), bf16),
            pltpu.VMEM((plan.tokens, 1), f32),
            pltpu.VMEM((plan.half, dl), f32),
            pltpu.VMEM((plan.half, dl), bf16),
            pltpu.VMEM((stages, plan.half, dl), bf16),
            pltpu.VMEM((stages * nx, plan.half, dl), bf16),
            pltpu.VMEM((stages * n, 8, LANES), f32),
            pltpu.VMEM((stages * n, 8, LANES), f32),
            dma((plan.blocks,)),
            dma((2, nch)),
            dma((2,)),
            dma((plan.layers,)),
            dma((2,)),
            dma((2, plan.ring * span)),
            dma((2,)),
            dma((2, plan.ring * span)),
            dma((2, LAST)),
            dma((1,)),
            dma((plan.blocks, n)),
            dma((1,)),
            dma((plan.blocks, n)),
            dma((1,)),
            dma((2, nx)),
            dma((2,)),
            dma((2,)),
            dma((1,)),
            dma((2,)),
        ],
        compiler_params=pltpu.CompilerParams(
            collective_id=0, has_side_effects=True, vmem_limit_bytes=58 * 1024 * 1024
        ),
        name="sublayers",
    )(*operands)


def local(
    n,
    nx,
    tokens,
    pre_gain,
    post_gain,
    gate_weight,
    up_weight,
    gate_taps,
    up_taps,
    gate_bias,
    up_bias,
    down_weight,
):
    layers, dl, fl = gate_weight.shape
    plan = Plan(layers, n, nx, tokens.shape[0], dl, fl, gate_taps.shape[1])
    return run(
        plan, tokens, pre_gain, post_gain, jnp.swapaxes(gate_taps, 0, 1), jnp.swapaxes(up_taps, 0, 1),
        gate_bias, up_bias, jnp.swapaxes(gate_weight, 1, 2), jnp.swapaxes(up_weight, 1, 2), down_weight)


def solution(mesh):
    in_specs = (
        P("grp", "ra"),
        P(None, "ra"),
        P(None, "ra"),
        P(None, "ra", "cb"),
        P(None, "ra", "cb"),
        P(None, None, "cb"),
        P(None, None, "cb"),
        P(None, "cb"),
        P(None, "cb"),
        P(None, "cb", "ra"),
    )
    body = functools.partial(local, mesh.shape["ra"], mesh.shape["cb"] // 2)
    return jax.shard_map(
        body, mesh=mesh, in_specs=in_specs, out_specs=P("grp", "ra"), check_vma=False
    )
```

```python
import functools

import jax
import jax.numpy as jnp
from jax import lax
from jax.experimental import pallas as pl
from jax.experimental.pallas import tpu as pltpu
from jax.sharding import PartitionSpec as P

LEN = 256
LANES = 128
BLOCK = 128
HALO = 8
HOP = 5
LAST = 4

epsilon = 1e-06
residual_scale = 0.5
MESH = pl.DeviceIdType.MESH


class Plan:
    def __init__(self, layers, n, nx, tokens, dl, fl, taps):
        self.layers, self.n, self.nx = layers, n, nx
        self.tokens, self.dl, self.fl = tokens, dl, fl
        self.side = taps + 1
        self.nfull = fl // LANES
        self.nch = -(-fl // LANES)
        self.tail = fl - self.nfull * LANES
        self.packed = 0 < 2 * self.tail <= LANES
        self.blocks = tokens // BLOCK
        self.per_seq = LEN // BLOCK
        self.span = -(-self.nch // 2)
        self.half = BLOCK // 2
        self.stages = layers * self.blocks
        self.tiles = [
            layers * sum(self.tiles_of(d, b) for b in range(self.blocks)) for d in range(2)]
        self.lasts = [
            sum(c // 2 >= self.span - LAST for c in self.chunks(d, self.blocks - 1)) for d in range(2)]
        self.hids = [
            layers * sum(len(self.chunks(d, b)) for b in range(self.blocks)) - self.lasts[d]
            for d in range(2)]
        assert n % 2 == 0
        self.turn = self.after(n - 1)
        self.done = self.after(2 * (n - 1))
        self.pair_at = self.done + 1
        self.x_at = self.pair_at + 5
        self.norm_at = self.x_at + 6
        self.next_at = self.norm_at + 1
        least = max(self.span + self.next_at + 1, (self.blocks - 1) * self.span + self.turn + 2)
        self.lap = max(self.blocks, -(-least // self.span))
        self.steps = ((layers - 1) * self.lap + self.blocks) * self.span + self.next_at + 1
        self.ring = -(-(HOP + 4) // self.span)

    def after(self, hops):
        return hops * HOP // 2

    def chunks(self, d, b):
        return range((d + b // self.per_seq) % 2, self.nch, 2)

    def tiles_of(self, d, b):
        chunks = self.chunks(d, b)
        return 2 * len(chunks) - (1 if self.packed and self.nfull in chunks else 0)


def body_kernel(
    plan,
    state_hbm, pre_ref, post_ref, gt_ref, ut_ref, gb_ref, ub_ref, wg_hbm, wu_hbm, wd_hbm,
    out_ref,
    gains, coefs, w, wd, part, hid, halo, acc, states, normed, scale, branch, pair_out, pair_in, xbuf, pre_sq, post_sq,
    ssem, wsem, wtail, wdsem, part_send, part_recv, hid_send, hid_recv, last_recv,
    pre_send, pre_recv, post_send, post_recv, x_send, x_recv, pair_send, pair_recv,
    back_send, back_recv,
):
    z = lax.axis_index("ra")
    k = lax.axis_index("cb")
    core, xi = k % 2, k // 2
    peer = k + 1 - 2 * core
    n, nx, layers, dl, fl = plan.n, plan.nx, plan.layers, plan.dl, plan.fl
    nch, nfull, tail, blocks, span, half = (
        plan.nch, plan.nfull, plan.tail, plan.blocks, plan.span, plan.half)
    width = dl * n
    f32 = jnp.float32

    def w_copies(layer, c):
        cols = pl.ds(pl.multiple_of(c * LANES, LANES), LANES)
        return (
            pltpu.make_async_copy(
                wg_hbm.at[layer, cols], w.at[c, pl.ds(0, LANES)], wsem.at[0, c]),
            pltpu.make_async_copy(
                wu_hbm.at[layer, cols], w.at[c, pl.ds(LANES, LANES)], wsem.at[1, c]),
        )

    up_at = tail if plan.packed else LANES

    def tail_copies(layer):
        cols = pl.ds(nfull * LANES, tail)
        return (
            pltpu.make_async_copy(
                wg_hbm.at[layer, cols], w.at[nfull, pl.ds(0, tail)], wtail.at[0]),
            pltpu.make_async_copy(
                wu_hbm.at[layer, cols], w.at[nfull, pl.ds(up_at, tail)], wtail.at[1]),
        )

    def w_do(layer, c, act):
        @pl.when(c < nfull)
        def _():
            for copy in w_copies(layer, c):
                act(copy)

        if tail:
            @pl.when(c == nfull)
            def _():
                for copy in tail_copies(layer):
                    act(copy)

    def start(copy):
        copy.start()

    def wait(copy):
        copy.wait()

    def wd_copy(layer):
        return pltpu.make_async_copy(
            wd_hbm.at[layer], wd.at[layer, pl.ds(0, fl)], wdsem.at[layer])

    def block_rows(b):
        return pl.ds(pl.multiple_of(b * BLOCK, BLOCK), BLOCK)

    def half_rows(b, which):
        return pl.ds(pl.multiple_of(b * BLOCK + which * half, half), half)

    def state_rows(layer, b):
        return block_rows(layer * blocks + b)

    def state_half(layer, b, which):
        return half_rows(layer * blocks + b, which)

    def state_copy(b):
        return pltpu.make_async_copy(
            state_hbm.at[block_rows(b)], states.at[block_rows(b)], ssem.at[b])

    barrier = pltpu.get_barrier_semaphore()

    @pl.loop(1, n)
    def _(o):
        pl.semaphore_signal(
            barrier, inc=1, device_id={"ra": (z + o) % n}, device_id_type=MESH)

    pl.semaphore_signal(barrier, inc=1, device_id={"cb": peer}, device_id_type=MESH)
    for o in range(1, nx):
        pl.semaphore_signal(
            barrier, inc=1, device_id={"cb": (xi + o) % nx * 2 + core}, device_id_type=MESH)

    for b in range(blocks):
        state_copy(b).start()

    @pl.loop(0, nch)
    def _(c):
        w_do(0, c, start)

    for layer in range(layers):
        wd_copy(layer).start()

    def eye(rows):
        shape = (rows, LANES)
        return lax.broadcasted_iota(jnp.int32, shape, 0) == lax.broadcasted_iota(
            jnp.int32, shape, 1)

    def to_row(column):
        return jnp.sum(jnp.where(eye(column.shape[0]), column, 0.0), axis=0, keepdims=True)

    def to_column(row, rows):
        return jnp.sum(jnp.where(eye(rows), row, 0.0), axis=1, keepdims=True)

    def sq_copy(buf, send, recv, t, o, slot):
        return pltpu.make_async_remote_copy(
            src_ref=buf.at[t * n + slot], dst_ref=buf.at[t * n + slot],
            send_sem=send.at[0], recv_sem=recv.at[t % blocks, slot],
            device_id={"ra": (z + o) % n}, device_id_type=MESH)

    def sq_start(buf, send, recv, t):
        @pl.loop(1, n)
        def _(o):
            sq_copy(buf, send, recv, t, o, z).start()

    def sq_wait(buf, send, recv, t):
        @pl.loop(1, n)
        def _(o):
            sq_copy(buf, send, recv, t, o, (z + o) % n).wait_recv()

    def scale_of(buf, t, rows):
        total = buf[t * n, 0:1, :]
        for slot in range(1, n):
            total = total + buf[t * n + slot, 0:1, :]
        return to_column(lax.rsqrt(total / width + epsilon), rows)

    def norm(layer, b):
        t = layer * blocks + b
        wide = states[state_rows(layer, b), :].astype(f32)
        normed[block_rows(b), :] = (wide * gains[layer, 0:1, :]).astype(normed.dtype)
        row = to_row(jnp.sum(wide * wide, axis=1, keepdims=True))
        pre_sq[t * n + z] = jnp.broadcast_to(row, pre_sq.shape[1:])

    if tail:
        for lo, hi in ((tail, up_at), (up_at + tail, 2 * LANES)):
            if lo < hi:
                w[nfull, lo:hi, :] = jnp.zeros((hi - lo, dl), w.dtype)
        for layer in range(layers):
            wd[layer, fl:, :] = jnp.zeros((nch * LANES - fl, dl), wd.dtype)

    taps = gt_ref.shape[0]
    side = taps + 1
    for layer in range(layers):
        gains[layer, 0:1, :] = pre_ref[layer : layer + 1, :].astype(f32)
        gains[layer, 1:2, :] = post_ref[layer : layer + 1, :].astype(f32)
    state_copy(0).wait()
    norm(0, 0)
    pl.semaphore_wait(barrier, n - 1 + nx)
    sq_start(pre_sq, pre_send, pre_recv, 0)

    def fill_coefs():
        if tail:
            coefs[:, :, nfull * LANES :] = jnp.zeros((layers, coefs.shape[1], LANES), f32)
        for at, (tap_ref, bias_ref) in ((0, (gt_ref, gb_ref)), (side, (ut_ref, ub_ref))):
            for i in range(side):
                both = (tap_ref[i] if i < taps else bias_ref[...]).astype(f32)
                for layer in range(layers):
                    coefs[layer, at + i : at + i + 1, 0:fl] = both[layer : layer + 1, :]
        if plan.packed:
            last = slice(nfull * LANES, (nfull + 1) * LANES)
            for layer in range(layers):
                for i in range(side):
                    up = coefs[layer, side + i : side + i + 1, last]
                    coefs[layer, i : i + 1, last] += pltpu.roll(up, tail, 1)

    def place(d):
        if d == 0:
            return n - 1 - z, z - 1, z + 1
        return z, z + 1, z - 1

    def part_tile(t, j, i):
        return (t * span + j) * 2 + i

    def part_do(d, t, j, c, target, act):
        def go(count):
            tiles = pl.ds(part_tile(t, j, 0), count)
            act(pltpu.make_async_remote_copy(
                src_ref=part.at[d, tiles], dst_ref=part.at[d, tiles],
                send_sem=part_send.at[d], recv_sem=part_recv.at[d, slot_of(t, j)],
                device_id={"ra": target}, device_id_type=MESH))

        if plan.packed:
            @pl.when(c < nfull)
            def _():
                go(2)

            @pl.when(c == nfull)
            def _():
                go(1)
        else:
            go(2)

    def wait_recv(copy):
        copy.wait_recv()

    def hid_copy(d, t, j, target):
        return pltpu.make_async_remote_copy(
            src_ref=hid.at[d, t * span + j], dst_ref=hid.at[d, t * span + j],
            send_sem=hid_send.at[d], recv_sem=hid_recv.at[d, slot_of(t, j)],
            device_id={"ra": target}, device_id_type=MESH)

    def last_copy(d, t, j, target):
        return pltpu.make_async_remote_copy(
            src_ref=hid.at[d, t * span + j], dst_ref=hid.at[d, t * span + j],
            send_sem=hid_send.at[d], recv_sem=last_recv.at[d, j - (span - LAST)],
            device_id={"ra": target}, device_id_type=MESH)

    def is_last(layer, b, j):
        return (layer == layers - 1) & (b == blocks - 1) & (j >= span - LAST)

    def one_of(b, members):
        return functools.reduce(jnp.logical_or, [b == i for i in members], jnp.bool_(False))

    def odd(b):
        return one_of(b, [i for i in range(blocks) if i // plan.per_seq % 2])

    def chunk_of(d, b, j):
        return 2 * j + jnp.where(odd(b), 1 - d, d)

    def slot_of(t, j):
        return j if plan.ring == 1 else t % plan.ring * span + j

    def advance(at, moving):
        layer, b, j = at
        j = j + jnp.where(moving, 1, 0)
        turn = j == span
        b = b + jnp.where(turn, 1, 0)
        lap = b == plan.lap
        return (
            layer + jnp.where(lap, 1, 0), jnp.where(lap, 0, b), jnp.where(turn, 0, j))

    def live_at(at, offset, s):
        layer, b, j = at
        live = (s >= offset) & (layer < layers)
        return live if plan.lap == blocks else live & (b < blocks)

    def ago(at, steps):
        layer, b, j = at
        laps = -(-steps // span)
        b = b - laps
        over = b < 0
        layer = jnp.where(over, layer - 1, layer)
        b = jnp.where(over, b + plan.lap, b)
        hit = (j == (span - 1 + steps) % span) & (layer >= 0) & (layer < layers)
        return hit if plan.lap == blocks else hit & (b < blocks), layer, b

    def conv(values, before, taps, bias):
        rows = lax.broadcasted_iota(jnp.int32, before.shape, 0)
        count = len(taps)
        result = taps[count - 1] * values
        for offset in range(1, count):
            moved = pltpu.roll(values, offset, 0)
            head = jnp.where(rows < offset, pltpu.roll(before, offset, 0), moved[:HALO])
            moved = jnp.concatenate([head, moved[HALO:]], axis=0)
            result = result + taps[count - 1 - offset] * moved
        return result + bias

    def wd_rows(c):
        return pl.ds(pl.multiple_of(c * LANES, LANES), LANES)

    def add_down(d, layer, b, j, c):
        at = (layer * blocks + b) * span + j

        @pl.when(j % 2 == 1)
        def _():
            two = jnp.concatenate([hid[d, at - 1], hid[d, at]], axis=1)
            rows = jnp.concatenate([wd[layer, wd_rows(c - 2), :], wd[layer, wd_rows(c), :]], axis=0)
            acc[block_rows(b), :] += jnp.dot(two, rows, preferred_element_type=f32)

        @pl.when((j % 2 == 0) & (c + 2 >= nch))
        def _():
            acc[block_rows(b), :] += jnp.dot(
                hid[d, at], wd[layer, wd_rows(c), :], preferred_element_type=f32)

    def pair_copy(t):
        return pltpu.make_async_remote_copy(
            src_ref=pair_out, dst_ref=pair_in.at[t],
            send_sem=pair_send.at[t % 2], recv_sem=pair_recv.at[t % 2],
            device_id={"cb": peer}, device_id_type=MESH)

    def x_copy(t, o, slot):
        return pltpu.make_async_remote_copy(
            src_ref=xbuf.at[t * nx + slot], dst_ref=xbuf.at[t * nx + slot],
            send_sem=x_send.at[0], recv_sem=x_recv.at[t % 2, slot],
            device_id={"cb": (xi + o) % nx * 2 + core}, device_id_type=MESH)

    def back_copy(layer, b, which):
        rows = state_half(layer + 1, b, which)
        t = layer * blocks + b
        return pltpu.make_async_remote_copy(
            src_ref=states.at[rows], dst_ref=states.at[rows],
            send_sem=back_send.at[0], recv_sem=back_recv.at[t % 2],
            device_id={"cb": peer}, device_id_type=MESH)

    offsets = [plan.turn, plan.done]
    halves = []
    for i in range(2):
        d = (z + 1 + i) % 2
        ahead = 2 * d - 1
        p = jnp.where(d == 1, z, n - 1 - z)
        halves.append((d, p, z + ahead, z - ahead))
        offsets += [plan.after(p), plan.after(2 * (n - 1) - p)]

    def step(s, streams):
        turn_at, done_at = streams[0], streams[1]
        sum_at, hid_at = streams[2::2], streams[3::2]

        @pl.when(s == 2)
        def _():
            fill_coefs()

        @pl.when((s >= 1) & (s < blocks))
        def _():
            state_copy(s).wait()
            norm(0, s)
            sq_start(pre_sq, pre_send, pre_recv, s)

        layer, b, j = turn_at

        @pl.when(live_at(turn_at, plan.turn, s) & (j == 0))
        def _():
            t = layer * blocks + b

            @pl.when(b == 0)
            def _():
                wd_copy(layer).wait()

            sq_wait(pre_sq, pre_send, pre_recv, t)
            scale[block_rows(b), :] = scale_of(pre_sq, t, BLOCK)
            acc[block_rows(b), :] = jnp.zeros((BLOCK, dl), f32)

        for i, (d, p, nxt, prv) in enumerate(halves):
            layer, b, j = sum_at[i]
            live = live_at(sum_at[i], plan.after(p), s)
            c = chunk_of(d, b, j)
            t = layer * blocks + b

            @pl.when(live & (c < nch))
            def _():
                @pl.when(b == 0)
                def _():
                    w_do(layer, c, wait)

                own = lax.dot_general(
                    normed[block_rows(b), :], w[c], (((1,), (1,)), ((), ())),
                    preferred_element_type=f32)

                def mine(i):
                    return own[:, i * LANES : (i + 1) * LANES]

                def tile(i):
                    return part[d, part_tile(t, j, i)].astype(f32)

                @pl.when(p == 0)
                def _():
                    for side_at in range(2):
                        part[d, part_tile(t, j, side_at)] = mine(side_at).astype(part.dtype)
                    part_do(d, t, j, c, nxt, start)

                @pl.when((p > 0) & (p < n - 1))
                def _():
                    part_do(d, t, j, c, nxt, wait_recv)
                    part[d, part_tile(t, j, 0)] = (tile(0) + mine(0)).astype(part.dtype)

                    @pl.when((c < nfull) | (not plan.packed))
                    def _():
                        part[d, part_tile(t, j, 1)] = (tile(1) + mine(1)).astype(part.dtype)

                    part_do(d, t, j, c, nxt, start)

                @pl.when(p == n - 1)
                def _():
                    part_do(d, t, j, c, prv, wait_recv)
                    coef = coefs[layer, :, wd_rows(c)]
                    row = [coef[i : i + 1, :] for i in range(2 * side)]
                    first = one_of(b, range(0, blocks, plan.per_seq))
                    last = plan.packed & (c == nfull)
                    sides = []
                    for k2 in range(2):
                        arrived = jnp.where(last, 0.0, tile(k2)) if k2 and plan.packed else tile(k2)
                        total = (arrived + mine(k2)) * scale[block_rows(b), :]
                        before = jnp.where(first, 0.0, halo[d, j, k2])
                        halo[d, j, k2] = total[BLOCK - HALO :, :]
                        at = k2 * side
                        sides.append(conv(total, before, row[at : at + taps], row[at + taps]))
                    gate, up = sides
                    if plan.packed:
                        up = jnp.where(last, pltpu.roll(gate, LANES - tail, 1), up)
                    value = jax.nn.gelu(gate, approximate=True) * up
                    if plan.packed:
                        lane = lax.broadcasted_iota(jnp.int32, value.shape, 1)
                        value = jnp.where(last & (lane >= tail), 0.0, value)
                    hid[d, t * span + j] = value.astype(hid.dtype)

                    @pl.when(jnp.logical_not(is_last(layer, b, j)))
                    def _():
                        hid_copy(d, t, j, prv).start()

                    @pl.when(is_last(layer, b, j))
                    def _():
                        for o in range(n - 1, 0, -1):
                            last_copy(d, t, j, z + o * (prv - z)).start()

                @pl.when((b == blocks - 1) & (layer + 1 < layers))
                def _():
                    w_do(layer + 1, c, start)

            layer, b, j = hid_at[i]
            live = live_at(hid_at[i], plan.after(2 * (n - 1) - p), s)
            c = chunk_of(d, b, j)
            t = layer * blocks + b

            @pl.when(live & (p < n - 1) & (c < nch))
            def _():
                @pl.when(jnp.logical_not(is_last(layer, b, j)))
                def _():
                    hid_copy(d, t, j, nxt).wait_recv()

                    @pl.when(p > 0)
                    def _():
                        hid_copy(d, t, j, prv).start()

                @pl.when(is_last(layer, b, j))
                def _():
                    last_copy(d, t, j, nxt).wait_recv()

            layer, b, j = hid_at[i]
            live = live_at(hid_at[i], plan.after(2 * (n - 1) - p), s)
            c = chunk_of(d, b, j)

            @pl.when(live & (c < nch))
            def _():
                add_down(d, layer, b, j, c)

        started = s >= plan.done
        hit, layer, b = ago(done_at, 0)

        @pl.when(started & hit)
        def _():
            t = layer * blocks + b
            pair_out[...] = acc[half_rows(b, 1 - core), :].astype(pair_out.dtype)
            pair_copy(t).start()

        hit, layer, b = ago(done_at, plan.pair_at - plan.done)

        @pl.when(started & hit)
        def _():
            t = layer * blocks + b
            pair_copy(t).wait()
            xbuf[t * nx + xi] = (
                acc[half_rows(b, core), :] + pair_in[t].astype(f32)).astype(xbuf.dtype)
            for o in range(1, nx):
                x_copy(t, o, xi).start()

        hit, layer, b = ago(done_at, plan.x_at - plan.done)

        @pl.when(started & hit)
        def _():
            t = layer * blocks + b
            for o in range(1, nx):
                x_copy(t, o, (xi + o) % nx).wait_recv()
            total = xbuf[t * nx].astype(f32)
            for i in range(1, nx):
                total = total + xbuf[t * nx + i].astype(f32)
            branch[...] = total
            row = to_row(jnp.sum(total * total, axis=1, keepdims=True))
            post_sq[t * n + z] = jnp.broadcast_to(row, post_sq.shape[1:])
            sq_start(post_sq, post_send, post_recv, t)

        hit, layer, b = ago(done_at, plan.norm_at - plan.done)

        @pl.when(started & hit)
        def _():
            t = layer * blocks + b
            sq_wait(post_sq, post_send, post_recv, t)
            states[state_half(layer + 1, b, core), :] = (
                residual_scale * states[state_half(layer, b, core), :].astype(f32)
                + branch[...] * scale_of(post_sq, t, half) * gains[layer, 1:2, :]
            ).astype(states.dtype)
            back_copy(layer, b, core).start()

        hit, layer, b = ago(done_at, plan.next_at - plan.done)

        @pl.when(started & hit)
        def _():
            t = layer * blocks + b
            back_copy(layer, b, 1 - core).wait_recv()

            @pl.when(layer + 1 < layers)
            def _():
                norm(layer + 1, b)
                sq_start(pre_sq, pre_send, pre_recv, t + blocks)

            @pl.when(layer + 1 == layers)
            def _():
                out_ref[block_rows(b), :] = states[state_rows(layers, b), :]

        return tuple(
            advance(at, s >= offset) for at, offset in zip(streams, offsets, strict=True))

    lax.fori_loop(0, plan.steps, step, tuple((jnp.int32(0),) * 3 for _ in offsets))

    def all_sent(buf, count, sem):
        sent = buf.at[pl.ds(0, count)]
        pltpu.make_async_remote_copy(
            src_ref=sent, dst_ref=sent, send_sem=sem, recv_sem=pair_recv.at[0],
            device_id={"cb": peer}, device_id_type=MESH).wait_send()

    all_sent(states, plan.stages * half, back_send.at[0])
    if nx > 1:
        all_sent(xbuf, plan.stages * (nx - 1), x_send.at[0])
    all_sent(pre_sq, plan.stages * (n - 1), pre_send.at[0])
    all_sent(post_sq, plan.stages * (n - 1), post_send.at[0])
    for d in range(2):
        p, nxt, prv = place(d)

        @pl.when(p < n - 1)
        def _():
            all_sent(part.at[d], plan.tiles[d], part_send.at[d])

        @pl.when(p > 0)
        def _():
            all_sent(hid.at[d], plan.hids[d], hid_send.at[d])

        @pl.when(p == n - 1)
        def _():
            for o in range(1, n):
                all_sent(hid.at[d], plan.lasts[d], hid_send.at[d])


def run(plan, *operands):
    vmem = pl.BlockSpec(memory_space=pltpu.VMEM)
    hbm = pl.BlockSpec(memory_space=pl.ANY)
    dma = pltpu.SemaphoreType.DMA
    bf16, f32 = jnp.bfloat16, jnp.float32
    n, nx, dl, nch, span, stages = plan.n, plan.nx, plan.dl, plan.nch, plan.span, plan.stages
    return pl.pallas_call(
        functools.partial(body_kernel, plan),
        out_shape=pltpu.VMEM((plan.tokens, dl), bf16),
        in_specs=[hbm] + [vmem] * 6 + [hbm] * 3,
        out_specs=vmem,
        scratch_shapes=[
            pltpu.VMEM((plan.layers, 2, dl), f32),
            pltpu.VMEM((plan.layers, 2 * plan.side, nch * LANES), f32),
            pltpu.VMEM((nch, 2 * LANES, dl), bf16),
            pltpu.VMEM((plan.layers, nch * LANES, dl), bf16),
            pltpu.VMEM((2, stages * span * 2, BLOCK, LANES), bf16),
            pltpu.VMEM((2, stages * span, BLOCK, LANES), bf16),
            pltpu.VMEM((2, span, 2, HALO, LANES), f32),
            pltpu.VMEM((plan.tokens, dl), f32),
            pltpu.VMEM(((plan.layers + 1) * plan.tokens, dl), bf16),
            pltpu.VMEM((plan.tokens, dl), bf16),
            pltpu.VMEM((plan.tokens, 1), f32),
            pltpu.VMEM((plan.half, dl), f32),
            pltpu.VMEM((plan.half, dl), bf16),
            pltpu.VMEM((stages, plan.half, dl), bf16),
            pltpu.VMEM((stages * nx, plan.half, dl), bf16),
            pltpu.VMEM((stages * n, 8, LANES), f32),
            pltpu.VMEM((stages * n, 8, LANES), f32),
            dma((plan.blocks,)),
            dma((2, nch)),
            dma((2,)),
            dma((plan.layers,)),
            dma((2,)),
            dma((2, plan.ring * span)),
            dma((2,)),
            dma((2, plan.ring * span)),
            dma((2, LAST)),
            dma((1,)),
            dma((plan.blocks, n)),
            dma((1,)),
            dma((plan.blocks, n)),
            dma((1,)),
            dma((2, nx)),
            dma((2,)),
            dma((2,)),
            dma((1,)),
            dma((2,)),
        ],
        compiler_params=pltpu.CompilerParams(
            collective_id=0, has_side_effects=True, vmem_limit_bytes=58 * 1024 * 1024
        ),
        name="sublayers",
    )(*operands)


def local(
    n,
    nx,
    tokens,
    pre_gain,
    post_gain,
    gate_weight,
    up_weight,
    gate_taps,
    up_taps,
    gate_bias,
    up_bias,
    down_weight,
):
    layers, dl, fl = gate_weight.shape
    plan = Plan(layers, n, nx, tokens.shape[0], dl, fl, gate_taps.shape[1])
    return run(
        plan, tokens, pre_gain, post_gain, jnp.swapaxes(gate_taps, 0, 1), jnp.swapaxes(up_taps, 0, 1),
        gate_bias, up_bias, jnp.swapaxes(gate_weight, 1, 2), jnp.swapaxes(up_weight, 1, 2), down_weight)


def solution(mesh):
    in_specs = (
        P("grp", "ra"),
        P(None, "ra"),
        P(None, "ra"),
        P(None, "ra", "cb"),
        P(None, "ra", "cb"),
        P(None, None, "cb"),
        P(None, None, "cb"),
        P(None, "cb"),
        P(None, "cb"),
        P(None, "cb", "ra"),
    )
    body = functools.partial(local, mesh.shape["ra"], mesh.shape["cb"] // 2)
    return jax.shard_map(
        body, mesh=mesh, in_specs=in_specs, out_specs=P("grp", "ra"), check_vma=False
    )
```
